32 devices in a mesh: sp: 16 (over z, y, core), tp: 2 (over x).
Axes of the slice: x: 2, y: 2, z: 4, core: 2. Of those that a mesh axis runs over, the one named last changes fastest.
Arguments:
- stream: bfloat16 [2048, 2048], P('sp', 'tp'), may hold values from -52 to 52
- norm_gain: float32 [2, 2048], replicated, may hold values from 0.1 to 1.9
- value_weight: bfloat16 [4096, 1024], P('sp', 'tp'), may hold values from -0.125 to 0.125
- gate_weight: bfloat16 [4096, 1024], P('sp', 'tp'), may hold values from -0.125 to 0.125
- conv_taps: float32 [2, 31, 1024], replicated, may hold values from -3 to 3
- ln_gain: float32 [2, 1024], replicated, may hold values from 0.1 to 1.9
- ln_bias: float32 [2, 1024], replicated, may hold values from -3 to 3
- out_weight: bfloat16 [1024, 4096], P('tp', 'sp'), may hold values from -0.1875 to 0.1875
- final_gain: float32 [2048], replicated, may hold values from 0.1 to 1.9
Outputs:
- result: bfloat16 [2048, 2048], P('sp', 'tp')
The draws below stay inside these ranges and needn't reach their ends.
All inputs are finite; a program needn't handle non-finite values.
Results may differ from the reference program's by a relative error of at most 0.014.
Values may be sent and summed in bfloat16 or wider, within the bound.
A program may use at most 64 MiB of HBM per device.

```python
import math
import jax
import jax.numpy as jnp
from jax import lax

D = 2048
C = 1024
KW = 31
LAYERS = 2
TOKENS = 2048
N_TP = 2


def draw_stream(key, part):
    key_values, key_rows, key_cols = jax.random.split(key, 3)
    column_place = jnp.arange(D, dtype=jnp.float32) / D - 0.5
    col_scale = jnp.exp(jnp.log(8.0) * column_place + jax.random.uniform(key_cols, (D,), jnp.float32, -0.35, 0.35))
    row_scale = jnp.exp(jax.random.uniform(key_rows, (TOKENS, 1), jnp.float32, -1.15, 1.15))
    values = jnp.clip(jax.random.normal(key_values, (TOKENS, D), jnp.float32), -4.0, 4.0)
    return (values * row_scale * col_scale).astype(jnp.bfloat16)


def draw_conv_taps(key, part):
    key_values, key_chans = jax.random.split(key)
    chan_place = jnp.arange(C, dtype=jnp.float32) / C - 0.5
    chan_scale = jnp.exp(jnp.log(6.0) * chan_place + jax.random.uniform(key_chans, (C,), jnp.float32, -0.35, 0.35))
    values = jnp.clip(jax.random.normal(key_values, (LAYERS, KW, C), jnp.float32), -4.0, 4.0)
    return (values * chan_scale / math.sqrt(KW)).astype(jnp.float32)


def level_of(stream_key, shape, shards, smallest, high):
    factor_of = 1.0
    for dim, blocks in shards:
        draws = jax.random.uniform(jax.random.fold_in(jax.random.fold_in(stream_key, 6), dim), (blocks,), jnp.float32, smallest / len(shards), high / len(shards))
        factor_of = factor_of * jnp.repeat(jnp.exp(draws), shape[dim] // blocks).reshape((-1,) + (1,) * (len(shape) - 1 - dim))
    return factor_of


def gaussian(own_key, dims, deviation, most, shards=(), held_as=jnp.bfloat16):
    factor_of = level_of(own_key, dims, shards, -0.22, 0.18) if shards else 1.0
    result = jax.random.normal(own_key, dims, jnp.float32) * deviation * factor_of
    return jnp.minimum(jnp.maximum(result, -most), most).astype(held_as)


def setup_inputs(seed: int = 0) -> dict:
    arg_keys = jax.random.split(jax.random.key(seed), 10)
    stream = draw_stream(jax.random.fold_in(arg_keys[9], 71), 0)
    norm_gain = jnp.clip(1.0 + 0.18 * jax.random.normal(arg_keys[1], (LAYERS, D), jnp.float32), 0.1, 1.9)
    value_weight = gaussian(arg_keys[2], (LAYERS * D, C), D ** -0.5, 0.125, ((0, 16), (1, 2)))
    gate_weight = gaussian(arg_keys[3], (LAYERS * D, C), D ** -0.5, 0.125, ((0, 16), (1, 2)))
    conv_taps = draw_conv_taps(jax.random.fold_in(arg_keys[9], 71), 0)
    ln_gain = jnp.clip(1.0 + 0.18 * jax.random.normal(arg_keys[5], (LAYERS, C), jnp.float32), 0.1, 1.9)
    ln_bias = gaussian(arg_keys[6], (LAYERS, C), 0.5, 3.0, (), jnp.float32)
    out_weight = gaussian(arg_keys[7], (C, LAYERS * D), C ** -0.5, 0.1875, ((0, 2), (1, 16)))
    final_gain = jnp.clip(1.0 + 0.18 * jax.random.normal(arg_keys[8], (D,), jnp.float32), 0.1, 1.9)
    return {"stream": stream, "norm_gain": norm_gain, "value_weight": value_weight, "gate_weight": gate_weight, "conv_taps": conv_taps, "ln_gain": ln_gain, "ln_bias": ln_bias, "out_weight": out_weight, "final_gain": final_gain}


EPS = 1e-06

def valid_conv(extended, tap_table):
    length = extended.shape[0] - (KW - 1)
    running = tap_table[0] * extended[0:length]
    for tap_index in range(1, KW):
        running = running + tap_table[tap_index] * extended[tap_index:tap_index + length]
    return running

def reference(stream, norm_gain, value_weight, gate_weight, conv_taps, ln_gain, ln_bias, out_weight, final_gain):
    value_all = value_weight.reshape(D, LAYERS, C)
    gate_all = gate_weight.reshape(D, LAYERS, C)
    out_all = out_weight.reshape(C, D, LAYERS)
    block_width = C // N_TP
    current = stream
    for layer_index in range(LAYERS):
        current32 = current.astype(jnp.float32)
        scale = lax.rsqrt(lax.optimization_barrier(jnp.sum(current32 * current32, axis=1, keepdims=True)) / D + EPS)
        normed = (current32 * scale * norm_gain[layer_index]).astype(jnp.bfloat16)
        value_proj = jnp.dot(normed, value_all[:, layer_index], preferred_element_type=jnp.float32)
        gate_proj = jnp.dot(normed, gate_all[:, layer_index], preferred_element_type=jnp.float32)
        glu_out = value_proj * jax.nn.sigmoid(gate_proj)
        extended = jnp.concatenate([jnp.zeros((KW - 1, C), jnp.float32), glu_out], axis=0)
        conv_out = valid_conv(extended, conv_taps[layer_index])
        row_mean = lax.optimization_barrier(jnp.sum(conv_out, axis=1, keepdims=True)) / C
        row_var = lax.optimization_barrier(jnp.sum(conv_out * conv_out, axis=1, keepdims=True)) / C - row_mean * row_mean
        active = jax.nn.silu((conv_out - row_mean) * lax.rsqrt(row_var + EPS) * ln_gain[layer_index] + ln_bias[layer_index]).astype(jnp.bfloat16)
        branch = jnp.zeros((current.shape[0], D), jnp.float32)
        for block_index in range(N_TP):
            low = block_index * block_width
            partial_value = jnp.dot(active[:, low:low + block_width], out_all[low:low + block_width, :, layer_index], preferred_element_type=jnp.float32)
            branch = branch + lax.optimization_barrier(partial_value.astype(jnp.bfloat16)).astype(jnp.float32)
        current = (current32 + branch).astype(jnp.bfloat16)
    final32 = current.astype(jnp.float32)
    squares = lax.optimization_barrier(jnp.sum(final32 * final32, axis=1, keepdims=True))
    return (final32 * lax.rsqrt(squares / D + EPS) * final_gain).astype(jnp.bfloat16)
```

```python
import functools

import jax
import jax.numpy as jnp
from jax import lax
from jax.experimental import pallas as pl
from jax.experimental.pallas import tpu as pltpu
from jax.sharding import PartitionSpec as P

D = 2048
C = 1024
KW = 31
LAYERS = 2


EPS = 1e-06


def from_behind(value, axis, steps):
    count = lax.axis_size(axis)
    first, last = (max(0, -steps), min(count, count - steps))
    return lax.ppermute(value, axis, [(source, source + steps) for source in range(first, last)])


def valid_conv(extended, tap_table):
    length = extended.shape[0] - (KW - 1)
    running = tap_table[0] * extended[0:length]
    for tap_index in range(1, KW):
        running = running + tap_table[tap_index] * extended[tap_index : tap_index + length]
    return running


def local(
    stream,
    norm_gain,
    value_weight,
    gate_weight,
    conv_taps,
    ln_gain,
    ln_bias,
    out_weight,
    final_gain,
):
    tokens_here = stream.shape[0]
    columns = stream.shape[1]
    channels = value_weight.shape[1]
    rim_rows = KW - 1
    tp_index = lax.axis_index("tp")
    my_taps = lax.dynamic_slice_in_dim(conv_taps, tp_index * channels, channels, 2)
    my_ln_gain = lax.dynamic_slice_in_dim(ln_gain, tp_index * channels, channels, 1)
    my_ln_bias = lax.dynamic_slice_in_dim(ln_bias, tp_index * channels, channels, 1)
    my_final = lax.dynamic_slice_in_dim(final_gain, tp_index * columns, columns, 0)
    value_all, gate_all, out_all = (
        lax.all_gather(value_weight, "sp", axis=0, tiled=True),
        lax.all_gather(gate_weight, "sp", axis=0, tiled=True),
        lax.all_gather(out_weight, "sp", axis=1, tiled=True),
    )
    value_all = value_all.reshape(D, LAYERS, channels)
    gate_all = gate_all.reshape(D, LAYERS, channels)
    out_all = out_all.reshape(channels, D, LAYERS)
    earlier = from_behind(stream[-LAYERS * rim_rows :], "sp", 1)
    current = jnp.concatenate([earlier, stream], axis=0)
    for layer_index in range(LAYERS):
        prefix = (LAYERS - layer_index) * rim_rows
        gathered = lax.all_gather(current, "tp", axis=1, tiled=True)
        gathered32 = gathered.astype(jnp.float32)
        scale = lax.rsqrt(jnp.sum(gathered32 * gathered32, axis=1, keepdims=True) / D + EPS)
        run_normed = (gathered32 * scale * norm_gain[layer_index]).astype(jnp.bfloat16)
        value_proj = jnp.dot(
            run_normed, value_all[:, layer_index], preferred_element_type=jnp.float32
        )
        gate_proj = jnp.dot(
            run_normed, gate_all[:, layer_index], preferred_element_type=jnp.float32
        )
        glu_out = value_proj * jax.nn.sigmoid(gate_proj)
        positions = (
            lax.axis_index("sp") * tokens_here - prefix + lax.iota(jnp.int32, current.shape[0])
        )
        extended = jnp.where((positions >= 0)[:, None], glu_out, 0.0)
        residual = current[rim_rows:].astype(jnp.float32)
        conv_out = valid_conv(extended, my_taps[layer_index])
        first_sums, square_sums = lax.psum(
            (jnp.sum(conv_out, axis=1), jnp.sum(conv_out * conv_out, axis=1)), "tp"
        )
        row_mean = (first_sums / C)[:, None]
        row_var = (square_sums / C)[:, None] - row_mean * row_mean
        run_active = jax.nn.silu(
            (conv_out - row_mean) * lax.rsqrt(row_var + EPS) * my_ln_gain[layer_index]
            + my_ln_bias[layer_index]
        ).astype(jnp.bfloat16)
        partial_value = jnp.dot(
            run_active, out_all[:, :, layer_index], preferred_element_type=jnp.float32
        )
        summed = lax.psum_scatter(
            partial_value.astype(jnp.bfloat16), "tp", scatter_dimension=1, tiled=True
        ).astype(jnp.float32)
        current = (residual + summed).astype(jnp.bfloat16)
    final32 = current.astype(jnp.float32)
    squares = lax.psum(jnp.sum(final32 * final32, axis=1), "tp")
    return (final32 * lax.rsqrt(squares[:, None] / D + EPS) * my_final).astype(jnp.bfloat16)


MESH = pl.DeviceIdType.MESH
HALO = 32


def fused_kernel(
    n, x_in, ng_in, v_in, g_in, taps_in, lng_in, lnb_in, o_in, fg_in, out_ref,
    ng_ref, v_ref, g_ref, taps_ref, lng_ref, lnb_ref, o_ref, fg_ref, isem,
    vg, gv, ob, osw, xs, x1, x2, x2r, nb, gl, ext, cv, cvs, cvr, act, st, rst,
    upsem, downsem, sidesem, coresem, xsem, vgsem, osem, swsem, xrsem, x1sem, x2sem, cvsem, glsem, hsem, tsem,
):
    levels = n // 4
    half_levels = levels // 2
    sp = lax.axis_index("sp")
    tp = lax.axis_index("tp")
    z, y, core = sp // 4, (sp // 2) % 2, sp % 2
    peer = 1 - tp
    rows, cols = xs.shape[2], xs.shape[3]
    depth, quarter = vg.shape[1], vg.shape[2] // 2
    width = ob.shape[3]
    has_up, has_down = z < levels - 1, z > 0
    swaps = tp + core == 1
    side, twin = sp + 2 - 4 * y, sp + 1 - 2 * core

    def index(zz, yy, cc):
        return (zz * 2 + yy) * 2 + cc

    loads = [
        pltpu.make_async_copy(source, to, isem.at[i])
        for i, (source, to) in enumerate((
            (v_in, v_ref), (g_in, g_ref), (x_in, xs.at[y, tp]), (o_in, o_ref), (ng_in, ng_ref),
            (taps_in, taps_ref), (lng_in, lng_ref), (lnb_in, lnb_ref), (fg_in, fg_ref)))
    ]
    for load in loads:
        load.start()

    def remote(src, dst, send, recv, to_sp, to_tp):
        return pltpu.make_async_remote_copy(
            src_ref=src, dst_ref=dst, send_sem=send, recv_sem=recv,
            device_id={"sp": to_sp, "tp": to_tp}, device_id_type=MESH)

    def same(ref, send, recv, to_sp):
        return remote(ref, ref, send, recv, to_sp, tp)

    barrier = pltpu.get_barrier_semaphore()

    def greet(to_sp, to_tp):
        pl.semaphore_signal(barrier, inc=1, device_id={"sp": to_sp, "tp": to_tp}, device_id_type=MESH)

    greet(side, tp)
    greet(twin, tp)
    greet(sp, peer)
    pl.when(has_up)(lambda: greet(sp + 4, tp))
    pl.when(has_down)(lambda: greet(sp - 4, tp))
    pl.when(swaps)(lambda: greet(twin, peer))
    before = sp - 1

    @pl.when(sp > 0)
    def _():
        for yy in range(2):
            greet(index(before // 4, yy, before % 2), tp)

    def follows(yy):
        return index(z, yy, core) + 1 < n

    def vg_copy(l, src, send, to_sp):
        return same(vg.at[l * n + src], send, vgsem.at[l, src], to_sp)

    def vg_give(l):
        return remote(gv.at[l], vg.at[l * n + sp], sidesem, vgsem.at[l, sp], side, tp)

    def vg_take(l, src):
        vg_copy(l, src, coresem, twin).wait_recv()

    def vg_up(l, src):
        pl.when(has_up)(lambda: vg_copy(l, src, upsem, sp + 4).start())

    def vg_down(l, src):
        pl.when(has_down)(lambda: vg_copy(l, src, downsem, sp - 4).start())

    def vg_core(l, src):
        vg_copy(l, src, coresem, twin).start()

    def vg_own(l):
        vg_up(l, sp)
        vg_down(l, sp)
        vg_core(l, sp)

    def vg_side(l):
        src = index(z, 1 - y, core)
        vg_take(l, src)
        vg_up(l, src)
        vg_down(l, src)
        vg_core(l, src)

    def vg_line(l, d):
        def one(zz, onward):
            for yy in (y, 1 - y):
                src = index(zz, yy, core)
                vg_take(l, src)
                onward(l, src)
                vg_core(l, src)

        pl.when(z - d >= 0)(lambda: one(z - d, vg_up))
        pl.when(z + d < levels)(lambda: one(z + d, vg_down))

    def vg_other(l):
        for zz in range(levels):
            for yy in range(2):
                vg_take(l, index(zz, yy, 1 - core))

    def o_copy(l, src, send, to_sp):
        return same(ob.at[l, src], send, osem.at[l, src], to_sp)

    def o_swap(l):
        return remote(osw.at[l], ob.at[l, twin], swsem.at[l, 0], swsem.at[l, 1], twin, peer)

    def o_own(l):
        pl.when(swaps)(lambda: o_swap(l).wait_recv())
        pl.when(has_up)(lambda: o_copy(l, sp, upsem, sp + 4).start())
        pl.when(has_down)(lambda: o_copy(l, sp, downsem, sp - 4).start())
        o_copy(l, sp, sidesem, side).start()
        o_copy(l, sp, coresem, twin).start()

    def o_line(l, d):
        def one(zz, up):
            src = index(zz, y, core)
            o_copy(l, src, coresem, twin).wait_recv()
            if up:
                pl.when(has_up)(lambda: o_copy(l, src, upsem, sp + 4).start())
            else:
                pl.when(has_down)(lambda: o_copy(l, src, downsem, sp - 4).start())
            o_copy(l, src, sidesem, side).start()
            o_copy(l, src, coresem, twin).start()

        pl.when(z - d >= 0)(lambda: one(z - d, True))
        pl.when(z + d < levels)(lambda: one(z + d, False))

    def o_across(l, zz):
        src = index(zz, 1 - y, core)
        o_copy(l, src, coresem, twin).wait_recv()
        o_copy(l, src, coresem, twin).start()

    def o_other(l, zz):
        for yy in range(2):
            o_copy(l, index(zz, yy, 1 - core), coresem, twin).wait_recv()

    lo = lax.broadcasted_iota(jnp.int32, (depth, LAYERS * depth), 0)
    hi = lax.broadcasted_iota(jnp.int32, (depth, LAYERS * depth), 1)
    clo = lax.broadcasted_iota(jnp.int32, (LAYERS * width, width), 1)
    chi = lax.broadcasted_iota(jnp.int32, (LAYERS * width, width), 0)

    def pick_rows(l):
        pick = (hi == LAYERS * lo + l).astype(jnp.float32).astype(jnp.bfloat16)
        for yy, keep in ((1 - y, False), (y, True)):
            here = pl.ds(pl.multiple_of(yy * quarter, 128), quarter)
            for kind, ref in enumerate((v_ref, g_ref)):
                picked = jnp.dot(pick, ref[:, here], preferred_element_type=jnp.float32).astype(jnp.bfloat16)
                if keep:
                    vg[l * n + sp, :, kind * quarter : (kind + 1) * quarter] = picked
                else:
                    gv[l, :, kind * quarter : (kind + 1) * quarter] = picked

    def pick_columns(l):
        pick = (chi == LAYERS * clo + l).astype(jnp.float32).astype(jnp.bfloat16)
        picked = jnp.dot(o_ref[...], pick, preferred_element_type=jnp.float32).astype(jnp.bfloat16)

        @pl.when(swaps)
        def _():
            osw[l] = picked
            o_swap(l).start()

        @pl.when(jnp.logical_not(swaps))
        def _():
            ob[l, sp] = picked

    def x_side():
        return same(xs.at[y, tp], sidesem, xrsem.at[0, 0], side)

    def x_peer(yy):
        return remote(xs.at[yy, tp], xs.at[yy, tp], xsem, xrsem.at[yy, 1], sp, peer)

    def square_sum(value):
        return jnp.sum(value * value, axis=1, keepdims=True)

    def normalise_first(yy):
        total = jnp.zeros((rows, 1), jnp.float32)
        for half in range(2):
            total = total + square_sum(xs[yy, half].astype(jnp.float32))
        scale = lax.rsqrt(total / D + EPS)
        for half in range(2):
            gain = ng_ref[0:1, half * cols : (half + 1) * cols]
            nb[yy, :, half * cols : (half + 1) * cols] = (
                xs[yy, half].astype(jnp.float32) * scale * gain).astype(jnp.bfloat16)

    def normalise_next(yy):
        total = jnp.zeros((rows, 1), jnp.float32)
        for half in range(2):
            for zz in range(levels):
                total = total + square_sum(x1[yy, half, zz].astype(jnp.float32))
        scale = lax.rsqrt(total / D + EPS)
        for half in range(2):
            for zz in range(levels):
                for part in range(2):
                    at = index(zz, part, half) * width
                    value = x1[yy, half, zz, :, part * width : (part + 1) * width].astype(jnp.float32)
                    nb[yy, :, at : at + width] = (
                        value * scale * ng_ref[1:2, at : at + width]).astype(jnp.bfloat16)

    def gl_copy(l):
        return remote(gl.at[l, 1 - y], ext.at[l, y, pl.ds(HALO, rows)], sidesem, glsem.at[l], side, tp)

    def halo(l, yy):
        return remote(
            gl.at[l, yy, pl.ds(rows - HALO, HALO)], ext.at[l, y, pl.ds(0, HALO)],
            hsem.at[l, 0, yy], hsem.at[l, 1, y], index(z, yy, core) + 1, tp)

    def halo_wait(l, q):
        remote(
            gl.at[l, 0, pl.ds(rows - HALO, HALO)], ext.at[l, q, pl.ds(0, HALO)],
            hsem.at[l, 0, 0], hsem.at[l, 1, q], side, tp).wait_recv()

    def glu(l):
        both = jnp.dot(
            nb[...].reshape(2 * rows, n * depth), vg[l * n : (l + 1) * n].reshape(n * depth, 2 * quarter),
            preferred_element_type=jnp.float32)
        out = both[:, :quarter] * jax.nn.sigmoid(both[:, quarter:])
        gl[l] = out.reshape(2, rows, quarter)
        for yy in range(2):
            pl.when(follows(yy))(lambda: halo(l, yy).start())
        gl_copy(l).start()
        ext[l, y, HALO:] = gl[l, y]

    def cv_copy(l, q):
        return remote(cvs.at[l, q], cvr.at[l, q], xsem, cvsem.at[l, q], sp, peer)

    def conv_rows(l, q, r0):
        tap_cols = pl.ds(pl.multiple_of((tp * 2 + q) * quarter, 128), quarter)
        running = jnp.zeros((HALO, quarter), jnp.float32)
        for k in range(KW):
            at = r0 + k + HALO - (KW - 1)
            running = running + taps_ref[k, l : l + 1, tap_cols] * ext[l, q, at : at + HALO]
        cv[q, r0 : r0 + HALO] = running
        cvs[l, q, r0 : r0 + HALO] = running.astype(jnp.bfloat16)

    def conv(l):
        for r0 in range(HALO, rows, HALO):
            conv_rows(l, y, r0)
        pl.when(sp > 0)(lambda: halo_wait(l, y))
        conv_rows(l, y, 0)
        cv_copy(l, y).start()
        gl_copy(l).wait_recv()
        for r0 in range(HALO, rows, HALO):
            conv_rows(l, 1 - y, r0)
        pl.when(sp > 0)(lambda: halo_wait(l, 1 - y))
        conv_rows(l, 1 - y, 0)
        cv_copy(l, 1 - y).start()

    def activate(l):
        first = jnp.zeros((rows, 1), jnp.float32)
        second = jnp.zeros((rows, 1), jnp.float32)
        for q in range(2):
            value = cv[q]
            first = first + jnp.sum(value, axis=1, keepdims=True)
            second = second + square_sum(value)
        for q in range(2):
            cv_copy(l, q).wait_recv()
            value = cvr[l, q].astype(jnp.float32)
            first = first + jnp.sum(value, axis=1, keepdims=True)
            second = second + square_sum(value)
        mean = first / C
        scale = lax.rsqrt(second / C - mean * mean + EPS)
        for half, source in ((tp, None), (peer, cvr)):
            for q in range(2):
                value = cv[q] if source is None else source[l, q].astype(jnp.float32)
                here = pl.ds(pl.multiple_of((half * 2 + q) * quarter, 128), quarter)
                v = (value - mean) * scale * lng_ref[l : l + 1, here] + lnb_ref[l : l + 1, here]
                act[half, :, q * quarter : (q + 1) * quarter] = (v / (1.0 + jnp.exp(-v))).astype(jnp.bfloat16)

    def branch(l, zz):
        total = None
        for cc in range(2):
            weights = jnp.concatenate([ob[l, index(zz, 0, cc)], ob[l, index(zz, 1, cc)]], axis=1)
            partial_sum = jnp.dot(act[cc], weights, preferred_element_type=jnp.float32)
            partial_sum = partial_sum.astype(jnp.bfloat16).astype(jnp.float32)
            total = partial_sum if total is None else total + partial_sum
        return total

    def x1_side(zz):
        return same(x1.at[y, tp, zz], sidesem, x1sem.at[0, 0, zz], side)

    def x1_peer(yy, zz):
        return remote(x1.at[yy, tp, zz], x1.at[yy, tp, zz], xsem, x1sem.at[yy, 1, zz], sp, peer)

    def step(i):
        return (z + levels + (1 - 2 * (z // half_levels)) * i) % levels

    def project_first(zz):
        o_across(0, zz)
        o_other(0, zz)
        added = branch(0, zz)
        for part in range(2):
            at = pl.ds(pl.multiple_of((index(zz, part, tp) % (n // 2)) * width, 128), width)
            here = xs[y, zz // half_levels, :, at].astype(jnp.float32)
            x1[y, tp, zz, :, part * width : (part + 1) * width] = (
                here + added[:, part * width : (part + 1) * width]).astype(jnp.bfloat16)
        x1_side(zz).start()
        x1_peer(y, zz).start()

    def x2_copy(zz):
        return remote(x2.at[zz], x2r.at[zz], xsem, x2sem.at[zz % half_levels], sp, peer)

    def project_last(zz):
        fresh = (x1[y, tp, zz].astype(jnp.float32) + branch(1, zz)).astype(jnp.bfloat16)
        x2[zz] = fresh
        pl.when(zz // half_levels == peer)(lambda: x2_copy(zz).start())
        return square_sum(fresh.astype(jnp.float32))

    def stat_copy():
        return remote(st, rst, tsem.at[0], tsem.at[1], sp, peer)

    loads[0].wait()
    loads[1].wait()
    pick_rows(0)

    @pl.when(sp == 0)
    def _():
        for l in range(LAYERS):
            for q in range(2):
                ext[l, q, 0:HALO] = jnp.zeros((HALO, quarter), jnp.float32)

    ends = [has_up, has_down, swaps, follows(0), follows(1)]
    pl.semaphore_wait(barrier, 3 + sum(end.astype(jnp.int32) for end in ends))

    vg_give(0).start()
    vg_own(0)
    loads[2].wait()
    x_peer(y).start()
    x_side().start()
    pick_rows(1)
    vg_give(1).start()
    loads[3].wait()
    for l in range(LAYERS):
        pick_columns(l)
    for load in loads[4:]:
        load.wait()
    vg_side(0)
    for d in range(1, levels - 1):
        vg_line(0, d)
        if d == 1:
            x_peer(y).wait_recv()
            normalise_first(y)
            x_side().wait_recv()
            x_peer(1 - y).start()
    o_own(0)
    vg_line(0, levels - 1)
    x_peer(1 - y).wait_recv()
    normalise_first(1 - y)
    vg_other(0)
    glu(0)
    for d in range(1, levels - 1):
        o_line(0, d)
    vg_own(1)
    vg_side(1)
    conv(0)
    o_line(0, levels - 1)
    activate(0)
    for i in range(levels):
        project_first(step(i))
        if i == 1:
            vg_line(1, 1)
    for d in range(2, levels - 1):
        vg_line(1, d)
    o_own(1)
    for i in range(levels):
        x1_side(step(i)).wait_recv()
        x1_peer(1 - y, step(i)).start()
    for i in range(levels):
        x1_peer(y, step(i)).wait_recv()
    normalise_next(y)
    for i in range(levels):
        x1_peer(1 - y, step(i)).wait_recv()
    normalise_next(1 - y)
    vg_line(1, levels - 1)
    vg_other(1)
    glu(1)
    for d in range(1, levels - 1):
        o_line(1, d)
    conv(1)
    activate(1)
    o_line(1, levels - 1)
    squares = jnp.zeros((rows, 1), jnp.float32)
    for i in range(levels):
        o_across(1, step(i))
        o_other(1, step(i))
        squares = squares + project_last(step(i))
    st[...] = jnp.broadcast_to(squares, (rows, 128)).T[0:8]
    stat_copy().start()

    for zz in range(levels):
        @pl.when(z == zz)
        def _():
            for sem, count in ((upsem, zz + 1 if zz < levels - 1 else 0), (downsem, levels - zz if zz > 0 else 0)):
                if count:
                    block = vg.at[0 : 3 * LAYERS * count]
                    pltpu.make_async_copy(block, block, sem).wait()
    for sem, count in ((coresem, 2 * n), (sidesem, LAYERS + LAYERS * levels + 2 + levels // 2 + LAYERS)):
        block = vg.at[0:count]
        pltpu.make_async_copy(block, block, sem).wait()
    for l in range(LAYERS):
        pl.when(swaps)(lambda: o_swap(l).wait_send())
        for yy in range(2):
            pl.when(follows(yy))(lambda: halo(l, yy).wait_send())

    stat_copy().wait_recv()
    both = st[...] + rst[...]
    total = jnp.concatenate([both] * (128 // 8), axis=0).T[:, 0:1]
    scale = lax.rsqrt(total / D + EPS)
    for i in range(half_levels):
        zz = tp * half_levels + i
        x2_copy(zz).wait_recv()
        for source, parity in ((x2, tp), (x2r, peer)):
            for part in range(2):
                at = ((i * 2 + part) * 2 + parity) * width
                gain = fg_ref[0:1, pl.ds(pl.multiple_of(tp * cols + at, 128), width)]
                value = source[zz, :, part * width : (part + 1) * width].astype(jnp.float32)
                out_ref[:, pl.ds(pl.multiple_of(at, 128), width)] = (value * scale * gain).astype(jnp.bfloat16)
    count = 4 + levels + LAYERS + levels // 4
    block = vg.at[0:count]
    pltpu.make_async_copy(block, block, xsem).wait()
    stat_copy().wait_send()


def fused(n, stream, norm_gain, value_weight, gate_weight, conv_taps, ln_gain, ln_bias, out_weight, final_gain):
    rows, cols = stream.shape
    depth, ch = value_weight.shape[0] // LAYERS, value_weight.shape[1]
    width = out_weight.shape[1] // LAYERS
    levels = n // 4
    bf16, f32 = jnp.bfloat16, jnp.float32
    dma = pltpu.SemaphoreType.DMA
    arrays = (stream, norm_gain, value_weight, gate_weight, conv_taps.transpose(1, 0, 2),
              ln_gain, ln_bias, out_weight, final_gain.reshape(1, -1))
    return pl.pallas_call(
        functools.partial(fused_kernel, n),
        out_shape=jax.ShapeDtypeStruct((rows, cols), bf16),
        in_specs=[pl.BlockSpec(memory_space=pl.ANY)] * 9,
        out_specs=pl.BlockSpec(memory_space=pltpu.VMEM),
        scratch_shapes=[pltpu.VMEM(array.shape, array.dtype) for array in arrays[1:]] + [
            dma((len(arrays),)),
            pltpu.VMEM((LAYERS * n, depth, ch), bf16),
            pltpu.VMEM((LAYERS, depth, ch), bf16),
            pltpu.VMEM((LAYERS, n, ch, width), bf16),
            pltpu.VMEM((LAYERS, ch, width), bf16),
            pltpu.VMEM((2, 2, rows, cols), bf16),
            pltpu.VMEM((2, 2, levels, rows, 2 * width), bf16),
            pltpu.VMEM((levels, rows, 2 * width), bf16),
            pltpu.VMEM((levels, rows, 2 * width), bf16),
            pltpu.VMEM((2, rows, 2 * cols), bf16),
            pltpu.VMEM((LAYERS, 2, rows, ch // 2), f32),
            pltpu.VMEM((LAYERS, 2, HALO + rows, ch // 2), f32),
            pltpu.VMEM((2, rows, ch // 2), f32),
            pltpu.VMEM((LAYERS, 2, rows, ch // 2), bf16),
            pltpu.VMEM((LAYERS, 2, rows, ch // 2), bf16),
            pltpu.VMEM((2, rows, ch), bf16),
            pltpu.VMEM((8, rows), f32),
            pltpu.VMEM((8, rows), f32),
            dma, dma, dma, dma, dma,
            dma((LAYERS, n)),
            dma((LAYERS, n)),
            dma((LAYERS, 2)),
            dma((2, 2)),
            dma((2, 2, levels)),
            dma((levels // 2,)),
            dma((LAYERS, 2)),
            dma((LAYERS,)),
            dma((LAYERS, 2, 2)),
            dma((2,)),
        ],
        compiler_params=pltpu.CompilerParams(collective_id=0, has_side_effects=True),
    )(*arrays)


def solution(mesh):
    placed = (P("sp", "tp"), P(), P("sp", "tp"), P("sp", "tp"), P(), P(), P(), P("tp", "sp"), P())
    n, n_tp = mesh.shape["sp"], mesh.shape["tp"]

    def step(*args):
        stream, out_weight = args[0], args[7]
        fits = (n_tp == 2 and n % 8 == 0 and stream.shape[0] == 128 and out_weight.shape[1] == 128 * LAYERS
                and args[2].shape == (128 * LAYERS, 512))
        return fused(n, *args) if fits else local(*args)

    return jax.shard_map(step, mesh=mesh, in_specs=placed, out_specs=P("sp", "tp"), check_vma=False)
```

```python
import functools

import jax
import jax.numpy as jnp
from jax import lax
from jax.experimental import pallas as pl
from jax.experimental.pallas import tpu as pltpu
from jax.sharding import PartitionSpec as P

D = 2048
C = 1024
KW = 31
LAYERS = 2


EPS = 1e-06


def from_behind(value, axis, steps):
    count = lax.axis_size(axis)
    first, last = (max(0, -steps), min(count, count - steps))
    return lax.ppermute(value, axis, [(source, source + steps) for source in range(first, last)])


def valid_conv(extended, tap_table):
    length = extended.shape[0] - (KW - 1)
    running = tap_table[0] * extended[0:length]
    for tap_index in range(1, KW):
        running = running + tap_table[tap_index] * extended[tap_index : tap_index + length]
    return running


def local(
    stream,
    norm_gain,
    value_weight,
    gate_weight,
    conv_taps,
    ln_gain,
    ln_bias,
    out_weight,
    final_gain,
):
    tokens_here = stream.shape[0]
    columns = stream.shape[1]
    channels = value_weight.shape[1]
    rim_rows = KW - 1
    tp_index = lax.axis_index("tp")
    my_taps = lax.dynamic_slice_in_dim(conv_taps, tp_index * channels, channels, 2)
    my_ln_gain = lax.dynamic_slice_in_dim(ln_gain, tp_index * channels, channels, 1)
    my_ln_bias = lax.dynamic_slice_in_dim(ln_bias, tp_index * channels, channels, 1)
    my_final = lax.dynamic_slice_in_dim(final_gain, tp_index * columns, columns, 0)
    value_all, gate_all, out_all = (
        lax.all_gather(value_weight, "sp", axis=0, tiled=True),
        lax.all_gather(gate_weight, "sp", axis=0, tiled=True),
        lax.all_gather(out_weight, "sp", axis=1, tiled=True),
    )
    value_all = value_all.reshape(D, LAYERS, channels)
    gate_all = gate_all.reshape(D, LAYERS, channels)
    out_all = out_all.reshape(channels, D, LAYERS)
    earlier = from_behind(stream[-LAYERS * rim_rows :], "sp", 1)
    current = jnp.concatenate([earlier, stream], axis=0)
    for layer_index in range(LAYERS):
        prefix = (LAYERS - layer_index) * rim_rows
        gathered = lax.all_gather(current, "tp", axis=1, tiled=True)
        gathered32 = gathered.astype(jnp.float32)
        scale = lax.rsqrt(jnp.sum(gathered32 * gathered32, axis=1, keepdims=True) / D + EPS)
        run_normed = (gathered32 * scale * norm_gain[layer_index]).astype(jnp.bfloat16)
        value_proj = jnp.dot(
            run_normed, value_all[:, layer_index], preferred_element_type=jnp.float32
        )
        gate_proj = jnp.dot(
            run_normed, gate_all[:, layer_index], preferred_element_type=jnp.float32
        )
        glu_out = value_proj * jax.nn.sigmoid(gate_proj)
        positions = (
            lax.axis_index("sp") * tokens_here - prefix + lax.iota(jnp.int32, current.shape[0])
        )
        extended = jnp.where((positions >= 0)[:, None], glu_out, 0.0)
        residual = current[rim_rows:].astype(jnp.float32)
        conv_out = valid_conv(extended, my_taps[layer_index])
        first_sums, square_sums = lax.psum(
            (jnp.sum(conv_out, axis=1), jnp.sum(conv_out * conv_out, axis=1)), "tp"
        )
        row_mean = (first_sums / C)[:, None]
        row_var = (square_sums / C)[:, None] - row_mean * row_mean
        run_active = jax.nn.silu(
            (conv_out - row_mean) * lax.rsqrt(row_var + EPS) * my_ln_gain[layer_index]
            + my_ln_bias[layer_index]
        ).astype(jnp.bfloat16)
        partial_value = jnp.dot(
            run_active, out_all[:, :, layer_index], preferred_element_type=jnp.float32
        )
        summed = lax.psum_scatter(
            partial_value.astype(jnp.bfloat16), "tp", scatter_dimension=1, tiled=True
        ).astype(jnp.float32)
        current = (residual + summed).astype(jnp.bfloat16)
    final32 = current.astype(jnp.float32)
    squares = lax.psum(jnp.sum(final32 * final32, axis=1), "tp")
    return (final32 * lax.rsqrt(squares[:, None] / D + EPS) * my_final).astype(jnp.bfloat16)


MESH = pl.DeviceIdType.MESH
HALO = 32


def fused_kernel(
    n, x_in, ng_in, v_in, g_in, taps_in, lng_in, lnb_in, o_in, fg_in, out_ref,
    ng_ref, v_ref, g_ref, taps_ref, lng_ref, lnb_ref, o_ref, fg_ref, isem,
    vg, gv, ob, osw, xs, x1, x2, x2r, nb, gl, gs, gr, ext, cv, cvs, cvr, act, st, rst,
    upsem, downsem, sidesem, coresem, xsem, gvsem, vgsem, osem, swsem, xrsem, x1sem, x2sem, cvsem, glsem, hsem, tsem,
):
    levels = n // 4
    half_levels = levels // 2
    sp = lax.axis_index("sp")
    tp = lax.axis_index("tp")
    z, y, core = sp // 4, (sp // 2) % 2, sp % 2
    peer = 1 - tp
    rows, cols = xs.shape[2], xs.shape[3]
    depth, quarter = vg.shape[1], vg.shape[2] // 2
    width = ob.shape[3]
    has_up, has_down = z < levels - 1, z > 0
    swaps = tp + core == 1
    side, twin = sp + 2 - 4 * y, sp + 1 - 2 * core

    def index(zz, yy, cc):
        return (zz * 2 + yy) * 2 + cc

    def remote(src, dst, send, recv, to_sp, to_tp):
        return pltpu.make_async_remote_copy(
            src_ref=src, dst_ref=dst, send_sem=send, recv_sem=recv,
            device_id={"sp": to_sp, "tp": to_tp}, device_id_type=MESH)

    def same(ref, send, recv, to_sp):
        return remote(ref, ref, send, recv, to_sp, tp)

    barrier = pltpu.get_barrier_semaphore()

    def greet(to_sp, to_tp):
        pl.semaphore_signal(barrier, inc=1, device_id={"sp": to_sp, "tp": to_tp}, device_id_type=MESH)

    greet(side, tp)
    greet(twin, tp)
    greet(sp, peer)
    pl.when(has_up)(lambda: greet(sp + 4, tp))
    pl.when(has_down)(lambda: greet(sp - 4, tp))
    pl.when(swaps)(lambda: greet(twin, peer))
    before = sp - 1

    @pl.when(sp > 0)
    def _():
        for yy in range(2):
            greet(index(before // 4, yy, before % 2), tp)

    loads = [
        pltpu.make_async_copy(source, to, isem.at[i])
        for i, (source, to) in enumerate((
            (v_in, v_ref), (g_in, g_ref), (x_in, xs.at[y, tp]), (o_in, o_ref), (ng_in, ng_ref),
            (taps_in, taps_ref), (lng_in, lng_ref), (lnb_in, lnb_ref), (fg_in, fg_ref)))
    ]
    for load in loads:
        load.start()

    def follows(yy):
        return index(z, yy, core) + 1 < n

    def vg_copy(l, src, send, to_sp):
        return same(vg.at[l * n + src], send, vgsem.at[l, src], to_sp)

    def vg_rows(half):
        return pl.ds(half * (depth // 2), depth // 2)

    def vg_give(l, half):
        return remote(gv.at[l, vg_rows(half)], vg.at[l * n + sp, vg_rows(half)], sidesem, gvsem.at[l, half], side, tp)

    def vg_take(l, src):
        vg_copy(l, src, coresem, twin).wait_recv()

    def vg_up(l, src):
        pl.when(has_up)(lambda: vg_copy(l, src, upsem, sp + 4).start())

    def vg_down(l, src):
        pl.when(has_down)(lambda: vg_copy(l, src, downsem, sp - 4).start())

    def vg_core(l, src):
        vg_copy(l, src, coresem, twin).start()

    def vg_own(l):
        vg_up(l, sp)
        vg_down(l, sp)
        vg_core(l, sp)

    def vg_side(l):
        src = index(z, 1 - y, core)
        for half in range(2):
            vg_give(l, half).wait_recv()
            block = vg.at[l * n + src, vg_rows(half)]
            pl.when(has_up)(lambda: same(block, upsem, vgsem.at[l, src], sp + 4).start())
            pl.when(has_down)(lambda: same(block, downsem, vgsem.at[l, src], sp - 4).start())
        vg_core(l, src)

    def vg_line(l, d):
        def one(zz, onward):
            for yy in (y, 1 - y):
                src = index(zz, yy, core)
                vg_take(l, src)
                onward(l, src)
                vg_core(l, src)

        pl.when(z - d >= 0)(lambda: one(z - d, vg_up))
        pl.when(z + d < levels)(lambda: one(z + d, vg_down))

    def vg_other(l):
        for zz in range(levels):
            for yy in range(2):
                vg_take(l, index(zz, yy, 1 - core))

    def o_copy(l, src, half, send, to_sp):
        block = ob.at[l, src, pl.ds(half * (ob.shape[2] // 2), ob.shape[2] // 2)]
        return same(block, send, osem.at[l, src, half], to_sp)

    def o_swap(l):
        return remote(osw.at[l], ob.at[l, twin], swsem.at[l, 0], swsem.at[l, 1], twin, peer)

    def o_take(l, src, half):
        o_copy(l, src, half, coresem, twin).wait_recv()

    def o_up(l, src, half):
        pl.when(has_up)(lambda: o_copy(l, src, half, upsem, sp + 4).start())

    def o_down(l, src, half):
        pl.when(has_down)(lambda: o_copy(l, src, half, downsem, sp - 4).start())

    def o_here(l, src, half):
        o_copy(l, src, half, sidesem, side).start()
        o_copy(l, src, half, coresem, twin).start()

    def o_own_line(l):
        for half in range(2):
            o_up(l, sp, half)
            o_down(l, sp, half)

    def o_own_here(l):
        for half in range(2):
            o_here(l, sp, half)

    def o_line(l, d):
        def one(zz, onward):
            src = index(zz, y, core)
            for half in range(2):
                o_take(l, src, half)
                onward(l, src, half)
                o_here(l, src, half)

        pl.when(z - d >= 0)(lambda: one(z - d, o_up))
        pl.when(z + d < levels)(lambda: one(z + d, o_down))

    def o_across(l, zz):
        src = index(zz, 1 - y, core)
        for half in range(2):
            o_take(l, src, half)
            o_copy(l, src, half, coresem, twin).start()

    def o_other(l, zz):
        for yy in range(2):
            for half in range(2):
                o_take(l, index(zz, yy, 1 - core), half)

    lo = lax.broadcasted_iota(jnp.int32, (depth, LAYERS * depth), 0)
    hi = lax.broadcasted_iota(jnp.int32, (depth, LAYERS * depth), 1)
    clo = lax.broadcasted_iota(jnp.int32, (LAYERS * width, width), 1)
    chi = lax.broadcasted_iota(jnp.int32, (LAYERS * width, width), 0)

    def pick_rows(l):
        pick = (hi == LAYERS * lo + l).astype(jnp.float32).astype(jnp.bfloat16)
        for yy, keep in ((1 - y, False), (y, True)):
            here = pl.ds(pl.multiple_of(yy * quarter, 128), quarter)
            for kind, ref in enumerate((v_ref, g_ref)):
                picked = jnp.dot(pick, ref[:, here], preferred_element_type=jnp.float32).astype(jnp.bfloat16)
                if keep:
                    vg[l * n + sp, :, kind * quarter : (kind + 1) * quarter] = picked
                else:
                    gv[l, :, kind * quarter : (kind + 1) * quarter] = picked

    def pick_columns(l):
        pick = (chi == LAYERS * clo + l).astype(jnp.float32).astype(jnp.bfloat16)
        picked = jnp.dot(o_ref[...], pick, preferred_element_type=jnp.float32).astype(jnp.bfloat16)

        @pl.when(swaps)
        def _():
            osw[l] = picked
            o_swap(l).start()

        @pl.when(jnp.logical_not(swaps))
        def _():
            ob[l, sp] = picked

    def x_side():
        return same(xs.at[y, tp], sidesem, xrsem.at[0, 0], side)

    def x_peer(yy):
        return remote(xs.at[yy, tp], xs.at[yy, tp], xsem, xrsem.at[yy, 1], sp, peer)

    def square_sum(value):
        return jnp.sum(value * value, axis=1, keepdims=True)

    def normalise_first(yy):
        total = jnp.zeros((rows, 1), jnp.float32)
        for half in range(2):
            total = total + square_sum(xs[yy, half].astype(jnp.float32))
        scale = lax.rsqrt(total / D + EPS)
        for half in range(2):
            gain = ng_ref[0:1, half * cols : (half + 1) * cols]
            nb[yy, :, half * cols : (half + 1) * cols] = (
                xs[yy, half].astype(jnp.float32) * scale * gain).astype(jnp.bfloat16)

    def normalise_next(yy):
        total = jnp.zeros((rows, 1), jnp.float32)
        for half in range(2):
            for zz in range(levels):
                total = total + square_sum(x1[yy, half, zz].astype(jnp.float32))
        scale = lax.rsqrt(total / D + EPS)
        for half in range(2):
            for zz in range(levels):
                for part in range(2):
                    at = index(zz, part, half) * width
                    value = x1[yy, half, zz, :, part * width : (part + 1) * width].astype(jnp.float32)
                    nb[yy, :, at : at + width] = (
                        value * scale * ng_ref[1:2, at : at + width]).astype(jnp.bfloat16)

    def gl_copy(l):
        return remote(gs.at[l], gr.at[l], sidesem, glsem.at[l], side, tp)

    def halo(l, yy):
        return remote(
            gl.at[l, yy, pl.ds(rows - HALO, HALO)], ext.at[l, y, pl.ds(0, HALO)],
            hsem.at[l, 0, yy], hsem.at[l, 1, y], index(z, yy, core) + 1, tp)

    def halo_wait(l, q):
        remote(
            gl.at[l, 0, pl.ds(rows - HALO, HALO)], ext.at[l, q, pl.ds(0, HALO)],
            hsem.at[l, 0, 0], hsem.at[l, 1, q], side, tp).wait_recv()

    def glu(l):
        both = jnp.dot(
            nb[...].reshape(2 * rows, n * depth), vg[l * n : (l + 1) * n].reshape(n * depth, 2 * quarter),
            preferred_element_type=jnp.float32)
        out = both[:, :quarter] * jax.nn.sigmoid(both[:, quarter:])
        gl[l] = out.reshape(2, rows, quarter)
        for yy in range(2):
            pl.when(follows(yy))(lambda: halo(l, yy).start())
        gs[l] = gl[l, 1 - y].astype(jnp.bfloat16)
        gl_copy(l).start()
        ext[l, y, HALO:] = gl[l, y]

    def cv_copy(l, q, half):
        here = pl.ds(half * (rows // 2), rows // 2)
        return remote(cvs.at[l, q, here], cvr.at[l, q, here], xsem, cvsem.at[l, q, half], sp, peer)

    def conv_rows(l, q, r0):
        tap_cols = pl.ds(pl.multiple_of((tp * 2 + q) * quarter, 128), quarter)
        running = jnp.zeros((HALO, quarter), jnp.float32)
        for k in range(KW):
            at = r0 + k + HALO - (KW - 1)
            running = running + taps_ref[k, l : l + 1, tap_cols] * ext[l, q, at : at + HALO]
        cv[q, r0 : r0 + HALO] = running
        cvs[l, q, r0 : r0 + HALO] = running.astype(jnp.bfloat16)

    def conv(l, q):
        for half in (1, 0):
            for r0 in range(half * rows // 2 + (HALO if half == 0 else 0), (half + 1) * rows // 2, HALO):
                conv_rows(l, q, r0)
            if half == 0:
                pl.when(sp > 0)(lambda: halo_wait(l, q))
                conv_rows(l, q, 0)
            cv_copy(l, q, half).start()

    def take_glu(l):
        gl_copy(l).wait_recv()
        ext[l, 1 - y, HALO:] = gr[l].astype(jnp.float32)

    def activate(l, between):
        first = jnp.zeros((rows, 1), jnp.float32)
        second = jnp.zeros((rows, 1), jnp.float32)
        for q in range(2):
            value = cv[q]
            first = first + jnp.sum(value, axis=1, keepdims=True)
            second = second + square_sum(value)
        for q in range(2):
            for half in range(2):
                cv_copy(l, q, half).wait_recv()
        between()
        for q in range(2):
            value = cvr[l, q].astype(jnp.float32)
            first = first + jnp.sum(value, axis=1, keepdims=True)
            second = second + square_sum(value)
        mean = first / C
        scale = lax.rsqrt(second / C - mean * mean + EPS)
        for half, source in ((tp, None), (peer, cvr)):
            for q in range(2):
                value = cv[q] if source is None else source[l, q].astype(jnp.float32)
                here = pl.ds(pl.multiple_of((half * 2 + q) * quarter, 128), quarter)
                v = (value - mean) * scale * lng_ref[l : l + 1, here] + lnb_ref[l : l + 1, here]
                act[half, :, q * quarter : (q + 1) * quarter] = (v / (1.0 + jnp.exp(-v))).astype(jnp.bfloat16)

    def branch(l, zz):
        total = None
        for cc in range(2):
            weights = jnp.concatenate([ob[l, index(zz, 0, cc)], ob[l, index(zz, 1, cc)]], axis=1)
            partial_sum = jnp.dot(act[cc], weights, preferred_element_type=jnp.float32)
            partial_sum = partial_sum.astype(jnp.bfloat16).astype(jnp.float32)
            total = partial_sum if total is None else total + partial_sum
        return total

    def x1_side(zz):
        return same(x1.at[y, tp, zz], sidesem, x1sem.at[0, 0, zz], side)

    def x1_peer(yy, zz):
        return remote(x1.at[yy, tp, zz], x1.at[yy, tp, zz], xsem, x1sem.at[yy, 1, zz], sp, peer)

    def x1_diagonal(zz):
        return same(x1.at[y, peer, zz], sidesem, x1sem.at[1, 0, zz], side)

    def step(i):
        return (z + levels + (1 - 2 * (z // half_levels)) * i) % levels

    def project_first(zz):
        o_other(0, zz)
        added = branch(0, zz)
        for part in range(2):
            at = pl.ds(pl.multiple_of((index(zz, part, tp) % (n // 2)) * width, 128), width)
            here = xs[y, zz // half_levels, :, at].astype(jnp.float32)
            x1[y, tp, zz, :, part * width : (part + 1) * width] = (
                here + added[:, part * width : (part + 1) * width]).astype(jnp.bfloat16)
        x1_side(zz).start()
        x1_peer(y, zz).start()

    def x2_copy(zz):
        return remote(x2.at[zz], x2r.at[zz], xsem, x2sem.at[zz % half_levels], sp, peer)

    def project_last(zz):
        fresh = (x1[y, tp, zz].astype(jnp.float32) + branch(1, zz)).astype(jnp.bfloat16)
        x2[zz] = fresh
        pl.when(zz // half_levels == peer)(lambda: x2_copy(zz).start())
        return square_sum(fresh.astype(jnp.float32))

    def stat_copy():
        return remote(st, rst, tsem.at[0], tsem.at[1], sp, peer)

    loads[0].wait()
    loads[1].wait()
    pick_rows(0)

    @pl.when(sp == 0)
    def _():
        for l in range(LAYERS):
            for q in range(2):
                ext[l, q, 0:HALO] = jnp.zeros((HALO, quarter), jnp.float32)

    ends = [has_up, has_down, swaps, follows(0), follows(1)]
    pl.semaphore_wait(barrier, 3 + sum(end.astype(jnp.int32) for end in ends))

    for half in range(2):
        vg_give(0, half).start()
    vg_own(0)
    loads[2].wait()
    x_peer(y).start()
    x_side().start()
    pick_rows(1)
    for half in range(2):
        vg_give(1, half).start()
    loads[3].wait()
    for l in range(LAYERS):
        pick_columns(l)
    keeps = jnp.logical_not(swaps)
    pl.when(keeps)(lambda: o_own_line(0))
    for load in loads[4:]:
        load.wait()
    vg_side(0)
    for d in range(1, levels - 1):
        vg_line(0, d)
        if d == 1:
            x_peer(y).wait_recv()
            normalise_first(y)
            x_side().wait_recv()
            x_peer(1 - y).start()
    @pl.when(swaps)
    def _():
        o_swap(0).wait_recv()
        o_own_line(0)

    o_own_here(0)
    vg_line(0, levels - 1)
    x_peer(1 - y).wait_recv()
    normalise_first(1 - y)
    vg_other(0)
    glu(0)
    middle = jnp.logical_and(has_up, has_down)
    last = jnp.logical_not(middle)

    def o_near(l, *distances):
        for d in distances:
            o_line(l, d)

    pl.when(middle)(lambda: o_near(0, *range(1, levels - 1)))
    vg_own(1)
    vg_side(1)
    conv(0, y)
    pl.when(last)(lambda: o_near(0, 1))
    take_glu(0)
    conv(0, 1 - y)
    o_across(0, step(0))
    pl.when(last)(lambda: o_near(0, *range(2, levels - 1)))

    def between(l):
        o_line(l, levels - 1)
        o_across(l, step(1))

    activate(0, lambda: between(0))
    project_first(step(0))
    o_across(0, step(2))
    project_first(step(1))
    pl.when(middle)(lambda: vg_line(1, 1))
    for i in range(2, levels):
        if i > 2:
            o_across(0, step(i))
        project_first(step(i))
    pl.when(last)(lambda: vg_line(1, 1))
    for i in range(levels):
        x1_side(step(i)).wait_recv()
        if i % 2 == 0:
            x1_peer(1 - y, step(i)).start()
        x1_peer(y, step(i)).wait_recv()
        if i % 2 == 1:
            x1_diagonal(step(i)).start()
    for d in range(2, levels - 1):
        vg_line(1, d)
    normalise_next(y)

    @pl.when(swaps)
    def _():
        o_swap(1).wait_recv()

    o_own_line(1)
    o_own_here(1)
    for i in range(levels):
        if i % 2 == 0:
            x1_peer(1 - y, step(i)).wait_recv()
        else:
            x1_diagonal(step(i)).wait_recv()
    normalise_next(1 - y)
    vg_line(1, levels - 1)
    vg_other(1)
    glu(1)
    pl.when(middle)(lambda: o_near(1, *range(1, levels - 1)))
    conv(1, y)
    pl.when(last)(lambda: o_near(1, 1))
    take_glu(1)
    conv(1, 1 - y)
    o_across(1, step(0))
    pl.when(last)(lambda: o_near(1, *range(2, levels - 1)))
    activate(1, lambda: between(1))
    squares = jnp.zeros((rows, 1), jnp.float32)
    for i in range(levels):
        if i > 0 and i < levels - 1:
            o_across(1, step(i + 1))
        o_other(1, step(i))
        squares = squares + project_last(step(i))
    st[...] = jnp.broadcast_to(squares, (rows, 128)).T[0:8]
    stat_copy().start()

    for zz in range(levels):
        @pl.when(z == zz)
        def _():
            for sem, count in ((upsem, zz + 1 if zz < levels - 1 else 0), (downsem, levels - zz if zz > 0 else 0)):
                if count:
                    block = vg.at[0 : 3 * LAYERS * count]
                    pltpu.make_async_copy(block, block, sem).wait()
    for sem, count in ((coresem, 2 * n), (sidesem, LAYERS + LAYERS * levels + 2 + levels // 2 + levels // 4 + LAYERS // 2)):
        block = vg.at[0:count]
        pltpu.make_async_copy(block, block, sem).wait()
    for l in range(LAYERS):
        pl.when(swaps)(lambda: o_swap(l).wait_send())
        for yy in range(2):
            pl.when(follows(yy))(lambda: halo(l, yy).wait_send())

    stat_copy().wait_recv()
    both = st[...] + rst[...]
    total = jnp.concatenate([both] * (128 // 8), axis=0).T[:, 0:1]
    scale = lax.rsqrt(total / D + EPS)
    for i in range(half_levels):
        zz = tp * half_levels + i
        x2_copy(zz).wait_recv()
        for source, parity in ((x2, tp), (x2r, peer)):
            for part in range(2):
                at = ((i * 2 + part) * 2 + parity) * width
                gain = fg_ref[0:1, pl.ds(pl.multiple_of(tp * cols + at, 128), width)]
                value = source[zz, :, part * width : (part + 1) * width].astype(jnp.float32)
                out_ref[:, pl.ds(pl.multiple_of(at, 128), width)] = (value * scale * gain).astype(jnp.bfloat16)
    count = 4 + levels // 2 + levels // 4 + LAYERS + levels // 4
    block = vg.at[0:count]
    pltpu.make_async_copy(block, block, xsem).wait()
    stat_copy().wait_send()


def fused(n, stream, norm_gain, value_weight, gate_weight, conv_taps, ln_gain, ln_bias, out_weight, final_gain):
    rows, cols = stream.shape
    depth, ch = value_weight.shape[0] // LAYERS, value_weight.shape[1]
    width = out_weight.shape[1] // LAYERS
    levels = n // 4
    bf16, f32 = jnp.bfloat16, jnp.float32
    dma = pltpu.SemaphoreType.DMA
    arrays = (stream, norm_gain, value_weight, gate_weight, conv_taps.transpose(1, 0, 2),
              ln_gain, ln_bias, out_weight, final_gain.reshape(1, -1))
    return pl.pallas_call(
        functools.partial(fused_kernel, n),
        out_shape=pltpu.VMEM((rows, cols), bf16),
        in_specs=[pl.BlockSpec(memory_space=pl.ANY)] * 9,
        out_specs=pl.BlockSpec(memory_space=pltpu.VMEM),
        scratch_shapes=[pltpu.VMEM(array.shape, array.dtype) for array in arrays[1:]] + [
            dma((len(arrays),)),
            pltpu.VMEM((LAYERS * n, depth, ch), bf16),
            pltpu.VMEM((LAYERS, depth, ch), bf16),
            pltpu.VMEM((LAYERS, n, ch, width), bf16),
            pltpu.VMEM((LAYERS, ch, width), bf16),
            pltpu.VMEM((2, 2, rows, cols), bf16),
            pltpu.VMEM((2, 2, levels, rows, 2 * width), bf16),
            pltpu.VMEM((levels, rows, 2 * width), bf16),
            pltpu.VMEM((levels, rows, 2 * width), bf16),
            pltpu.VMEM((2, rows, 2 * cols), bf16),
            pltpu.VMEM((LAYERS, 2, rows, ch // 2), f32),
            pltpu.VMEM((LAYERS, rows, ch // 2), bf16),
            pltpu.VMEM((LAYERS, rows, ch // 2), bf16),
            pltpu.VMEM((LAYERS, 2, HALO + rows, ch // 2), f32),
            pltpu.VMEM((2, rows, ch // 2), f32),
            pltpu.VMEM((LAYERS, 2, rows, ch // 2), bf16),
            pltpu.VMEM((LAYERS, 2, rows, ch // 2), bf16),
            pltpu.VMEM((2, rows, ch), bf16),
            pltpu.VMEM((8, rows), f32),
            pltpu.VMEM((8, rows), f32),
            dma, dma, dma, dma, dma,
            dma((LAYERS, 2)),
            dma((LAYERS, n)),
            dma((LAYERS, n, 2)),
            dma((LAYERS, 2)),
            dma((2, 2)),
            dma((2, 2, levels)),
            dma((levels // 2,)),
            dma((LAYERS, 2, 2)),
            dma((LAYERS,)),
            dma((LAYERS, 2, 2)),
            dma((2,)),
        ],
        compiler_params=pltpu.CompilerParams(collective_id=0, has_side_effects=True),
    )(*arrays)


def solution(mesh):
    placed = (P("sp", "tp"), P(), P("sp", "tp"), P("sp", "tp"), P(), P(), P(), P("tp", "sp"), P())
    n, n_tp = mesh.shape["sp"], mesh.shape["tp"]

    def step(*args):
        stream, out_weight = args[0], args[7]
        fits = (n_tp == 2 and n % 8 == 0 and stream.shape[0] == 128 and out_weight.shape[1] == 128 * LAYERS
                and args[2].shape == (128 * LAYERS, 512))
        return fused(n, *args) if fits else local(*args)

    return jax.shard_map(step, mesh=mesh, in_specs=placed, out_specs=P("sp", "tp"), check_vma=False)
```

```python
import functools

import jax
import jax.numpy as jnp
from jax import lax
from jax.experimental import pallas as pl
from jax.experimental.pallas import tpu as pltpu
from jax.sharding import PartitionSpec as P

D = 2048
C = 1024
KW = 31
LAYERS = 2


EPS = 1e-06


def from_behind(value, axis, steps):
    count = lax.axis_size(axis)
    first, last = (max(0, -steps), min(count, count - steps))
    return lax.ppermute(value, axis, [(source, source + steps) for source in range(first, last)])


def valid_conv(extended, tap_table):
    length = extended.shape[0] - (KW - 1)
    running = tap_table[0] * extended[0:length]
    for tap_index in range(1, KW):
        running = running + tap_table[tap_index] * extended[tap_index : tap_index + length]
    return running


def local(
    stream,
    norm_gain,
    value_weight,
    gate_weight,
    conv_taps,
    ln_gain,
    ln_bias,
    out_weight,
    final_gain,
):
    tokens_here = stream.shape[0]
    columns = stream.shape[1]
    channels = value_weight.shape[1]
    rim_rows = KW - 1
    tp_index = lax.axis_index("tp")
    my_taps = lax.dynamic_slice_in_dim(conv_taps, tp_index * channels, channels, 2)
    my_ln_gain = lax.dynamic_slice_in_dim(ln_gain, tp_index * channels, channels, 1)
    my_ln_bias = lax.dynamic_slice_in_dim(ln_bias, tp_index * channels, channels, 1)
    my_final = lax.dynamic_slice_in_dim(final_gain, tp_index * columns, columns, 0)
    value_all, gate_all, out_all = (
        lax.all_gather(value_weight, "sp", axis=0, tiled=True),
        lax.all_gather(gate_weight, "sp", axis=0, tiled=True),
        lax.all_gather(out_weight, "sp", axis=1, tiled=True),
    )
    value_all = value_all.reshape(D, LAYERS, channels)
    gate_all = gate_all.reshape(D, LAYERS, channels)
    out_all = out_all.reshape(channels, D, LAYERS)
    earlier = from_behind(stream[-LAYERS * rim_rows :], "sp", 1)
    current = jnp.concatenate([earlier, stream], axis=0)
    for layer_index in range(LAYERS):
        prefix = (LAYERS - layer_index) * rim_rows
        gathered = lax.all_gather(current, "tp", axis=1, tiled=True)
        gathered32 = gathered.astype(jnp.float32)
        scale = lax.rsqrt(jnp.sum(gathered32 * gathered32, axis=1, keepdims=True) / D + EPS)
        run_normed = (gathered32 * scale * norm_gain[layer_index]).astype(jnp.bfloat16)
        value_proj = jnp.dot(
            run_normed, value_all[:, layer_index], preferred_element_type=jnp.float32
        )
        gate_proj = jnp.dot(
            run_normed, gate_all[:, layer_index], preferred_element_type=jnp.float32
        )
        glu_out = value_proj * jax.nn.sigmoid(gate_proj)
        positions = (
            lax.axis_index("sp") * tokens_here - prefix + lax.iota(jnp.int32, current.shape[0])
        )
        extended = jnp.where((positions >= 0)[:, None], glu_out, 0.0)
        residual = current[rim_rows:].astype(jnp.float32)
        conv_out = valid_conv(extended, my_taps[layer_index])
        first_sums, square_sums = lax.psum(
            (jnp.sum(conv_out, axis=1), jnp.sum(conv_out * conv_out, axis=1)), "tp"
        )
        row_mean = (first_sums / C)[:, None]
        row_var = (square_sums / C)[:, None] - row_mean * row_mean
        run_active = jax.nn.silu(
            (conv_out - row_mean) * lax.rsqrt(row_var + EPS) * my_ln_gain[layer_index]
            + my_ln_bias[layer_index]
        ).astype(jnp.bfloat16)
        partial_value = jnp.dot(
            run_active, out_all[:, :, layer_index], preferred_element_type=jnp.float32
        )
        summed = lax.psum_scatter(
            partial_value.astype(jnp.bfloat16), "tp", scatter_dimension=1, tiled=True
        ).astype(jnp.float32)
        current = (residual + summed).astype(jnp.bfloat16)
    final32 = current.astype(jnp.float32)
    squares = lax.psum(jnp.sum(final32 * final32, axis=1), "tp")
    return (final32 * lax.rsqrt(squares[:, None] / D + EPS) * my_final).astype(jnp.bfloat16)


MESH = pl.DeviceIdType.MESH
HALO = 32


def fused_kernel(
    n, x_in, ng_in, v_in, g_in, taps_in, lng_in, lnb_in, o_in, fg_in, out_ref,
    ng_ref, v_ref, g_ref, taps_ref, lng_ref, lnb_ref, o_ref, fg_ref, isem,
    vg, gv, ob, osw, xs, x1, x2, x2r, nb, gl, gs, gr, ext, cv, cvs, cvr, act, st, rst,
    upsem, downsem, sidesem, coresem, xsem, gvsem, vgsem, vcsem, osem, ocsem, swsem, xrsem, x1sem, x2sem, cvsem, glsem, hssem, hsem, tsem,
):
    levels = n // 4
    half_levels = levels // 2
    sp = lax.axis_index("sp")
    tp = lax.axis_index("tp")
    z, y, core = sp // 4, (sp // 2) % 2, sp % 2
    peer = 1 - tp
    rows, cols = xs.shape[2], xs.shape[3]
    depth, quarter = vg.shape[1], vg.shape[2] // 2
    width = ob.shape[3]
    has_up, has_down = z < levels - 1, z > 0
    swaps = tp + core == 1
    side, twin = sp + 2 - 4 * y, sp + 1 - 2 * core

    def index(zz, yy, cc):
        return (zz * 2 + yy) * 2 + cc

    def landed(block, sem):
        pltpu.make_async_copy(block, block, sem).wait()

    def remote(src, dst, send, recv, to_sp, to_tp):
        return pltpu.make_async_remote_copy(
            src_ref=src, dst_ref=dst, send_sem=send, recv_sem=recv,
            device_id={"sp": to_sp, "tp": to_tp}, device_id_type=MESH)

    def same(ref, send, recv, to_sp):
        return remote(ref, ref, send, recv, to_sp, tp)

    barrier = pltpu.get_barrier_semaphore()

    def greet(to_sp, to_tp):
        pl.semaphore_signal(barrier, inc=1, device_id={"sp": to_sp, "tp": to_tp}, device_id_type=MESH)

    greet(side, tp)
    greet(twin, tp)
    greet(sp, peer)
    pl.when(has_up)(lambda: greet(sp + 4, tp))
    pl.when(has_down)(lambda: greet(sp - 4, tp))
    pl.when(swaps)(lambda: greet(twin, peer))
    before = sp - 1

    @pl.when(sp > 0)
    def _():
        for yy in range(2):
            greet(index(before // 4, yy, before % 2), tp)

    loads = [
        pltpu.make_async_copy(source, to, isem.at[max(i - 1, 0)])
        for i, (source, to) in enumerate((
            (v_in, v_ref), (g_in, g_ref), (x_in, xs.at[y, tp]), (o_in, o_ref), (ng_in, ng_ref),
            (taps_in, taps_ref), (lng_in, lng_ref), (lnb_in, lnb_ref), (fg_in, fg_ref)))
    ]
    for load in loads:
        load.start()

    def follows(yy):
        return index(z, yy, core) + 1 < n

    def vg_copy(l, src, send, to_sp):
        return same(vg.at[l * n + src], send, vgsem.at[l, src // 2], to_sp)

    def gives(l):
        return 2 if l == 0 else 1

    def vg_rows(l, half):
        return pl.ds(half * (depth // gives(l)), depth // gives(l))

    def vg_give(l, half):
        here = vg_rows(l, half)
        return remote(
            gv.at[l, here], vg.at[l * n + sp, here], sidesem, gvsem.at[half if l == 0 else l + 1], side, tp)

    def vg_take(l, src):
        vg_copy(l, src, coresem, twin).wait_recv()

    def vg_up(l, src):
        pl.when(has_up)(lambda: vg_copy(l, src, upsem, sp + 4).start())

    def vg_down(l, src):
        pl.when(has_down)(lambda: vg_copy(l, src, downsem, sp - 4).start())

    def vg_core(l, src):
        same(vg.at[l * n + src], coresem, vcsem.at[l], twin).start()

    def vg_own(l):
        vg_up(l, sp)
        vg_down(l, sp)
        vg_core(l, sp)

    def vg_side(l):
        src = index(z, 1 - y, core)
        for half in range(gives(l)):
            vg_give(l, half).wait_recv()
            block = vg.at[l * n + src, vg_rows(l, half)]
            pl.when(has_up)(lambda: same(block, upsem, vgsem.at[l, src // 2], sp + 4).start())
            pl.when(has_down)(lambda: same(block, downsem, vgsem.at[l, src // 2], sp - 4).start())
        vg_core(l, src)

    def vg_line(l, d):
        def one(zz, onward):
            for yy in (y, 1 - y):
                src = index(zz, yy, core)
                vg_take(l, src)
                onward(l, src)
                vg_core(l, src)

        pl.when(z - d >= 0)(lambda: one(z - d, vg_up))
        pl.when(z + d < levels)(lambda: one(z + d, vg_down))

    def vg_other(l):
        landed(vg.at[0 : n // 2], vcsem.at[l])

    def halves(l):
        return range(2 if l == LAYERS - 1 else 1)

    def o_block(l, src, half):
        size = ob.shape[2] // len(halves(l))
        return ob.at[l, src, pl.ds(half * size, size)]

    def o_copy(l, src, half, send, to_sp):
        at = src // 2 if l == 0 else n // 2 + src // 2 * 2 + half
        return same(o_block(l, src, half), send, osem.at[at], to_sp)

    def o_core(l, src, half):
        at = src // 4 if l == 0 else levels + src // 2
        same(o_block(l, src, half), coresem, ocsem.at[at], twin).start()

    def o_swap(l):
        return remote(osw.at[l], ob.at[l, twin], swsem.at[0], swsem.at[1 + l], twin, peer)

    def o_take(l, src, half):
        o_copy(l, src, half, sidesem, side).wait_recv()

    def o_up(l, src, half):
        pl.when(has_up)(lambda: o_copy(l, src, half, upsem, sp + 4).start())

    def o_down(l, src, half):
        pl.when(has_down)(lambda: o_copy(l, src, half, downsem, sp - 4).start())

    def o_here(l, src, half):
        o_copy(l, src, half, sidesem, side).start()
        o_core(l, src, half)

    def o_swapped(l):
        pl.when(swaps)(lambda: o_swap(l).wait_recv())

    def o_own_line(l, up, down):
        for half in halves(l):
            pl.when(up)(lambda: o_up(l, sp, half))
            pl.when(down)(lambda: o_down(l, sp, half))

    def o_own_here(l):
        for half in halves(l):
            o_here(l, sp, half)

    def o_line(l, d):
        def one(zz, onward):
            src = index(zz, y, core)
            for half in halves(l):
                o_take(l, src, half)
                onward(l, src, half)
                o_here(l, src, half)

        pl.when(z - d >= 0)(lambda: one(z - d, o_up))
        pl.when(z + d < levels)(lambda: one(z + d, o_down))

    def o_across(l, zz):
        src = index(zz, 1 - y, core)
        for half in halves(l):
            o_take(l, src, half)
            o_core(l, src, half)

    def o_other_both(zz):
        landed(ob.at[0, 0:2], ocsem.at[zz])

    def o_other(zz, yy):
        landed(ob.at[0, 0], ocsem.at[levels + zz * 2 + yy])

    lo = lax.broadcasted_iota(jnp.int32, (depth, LAYERS * depth), 0)
    hi = lax.broadcasted_iota(jnp.int32, (depth, LAYERS * depth), 1)
    clo = lax.broadcasted_iota(jnp.int32, (LAYERS * width, width), 1)
    chi = lax.broadcasted_iota(jnp.int32, (LAYERS * width, width), 0)

    def pick_rows(l):
        pick = (hi == LAYERS * lo + l).astype(jnp.float32).astype(jnp.bfloat16)
        for yy, keep in ((1 - y, False), (y, True)):
            here = pl.ds(pl.multiple_of(yy * quarter, 128), quarter)
            for kind, ref in enumerate((v_ref, g_ref)):
                picked = jnp.dot(pick, ref[:, here], preferred_element_type=jnp.float32).astype(jnp.bfloat16)
                at = kind * quarter
                if keep:
                    vg[l * n + sp, :, at : at + quarter] = picked
                else:
                    gv[l, :, at : at + quarter] = picked

    def pick_columns(l):
        pick = (chi == LAYERS * clo + l).astype(jnp.float32).astype(jnp.bfloat16)
        picked = jnp.dot(o_ref[...], pick, preferred_element_type=jnp.float32).astype(jnp.bfloat16)

        @pl.when(swaps)
        def _():
            osw[l] = picked
            o_swap(l).start()

        @pl.when(jnp.logical_not(swaps))
        def _():
            ob[l, sp] = picked

    def x_side():
        return same(xs.at[y, tp], sidesem, xrsem.at[0], side)

    def x_peer(far):
        block = xs.at[1 - y if far else y, tp]
        return remote(block, block, xsem, xrsem.at[1 + far], sp, peer)

    def square_sum(value):
        return jnp.sum(value * value, axis=1, keepdims=True)

    def normalise_first(yy):
        total = jnp.zeros((rows, 1), jnp.float32)
        for half in range(2):
            total = total + square_sum(xs[yy, half].astype(jnp.float32))
        scale = lax.rsqrt(total / D + EPS)
        for half in range(2):
            gain = ng_ref[0:1, half * cols : (half + 1) * cols]
            nb[yy, :, half * cols : (half + 1) * cols] = (
                xs[yy, half].astype(jnp.float32) * scale * gain).astype(jnp.bfloat16)

    def normalise_next(yy):
        total = jnp.zeros((rows, 1), jnp.float32)
        for half in range(2):
            for zz in range(levels):
                for part in range(2):
                    total = total + square_sum(x1[yy, half, zz, part].astype(jnp.float32))
        scale = lax.rsqrt(total / D + EPS)
        for half in range(2):
            for zz in range(levels):
                for part in range(2):
                    at = index(zz, part, half) * width
                    value = x1[yy, half, zz, part].astype(jnp.float32)
                    nb[yy, :, at : at + width] = (
                        value * scale * ng_ref[1:2, at : at + width]).astype(jnp.bfloat16)

    def gl_copy(l, half):
        here = pl.ds(half * (rows // 2), rows // 2)
        return remote(gs.at[l, here], gr.at[l, here], sidesem, glsem.at[l], side, tp)

    def halo(l, yy):
        return remote(
            gl.at[l, yy], ext.at[l, y, pl.ds(0, HALO)],
            hssem.at[yy], hsem.at[l, y], index(z, yy, core) + 1, tp)

    def halo_wait(l, q):
        remote(
            gl.at[l, 0], ext.at[l, q, pl.ds(0, HALO)],
            hssem.at[0], hsem.at[l, q], side, tp).wait_recv()

    def glu(l):
        weights = vg[l * n : (l + 1) * n].reshape(n * depth, 2 * quarter)

        def tokens(yy):
            both = jnp.dot(nb[yy], weights, preferred_element_type=jnp.float32)
            return both[:, :quarter] * jax.nn.sigmoid(both[:, quarter:])

        theirs = tokens(1 - y)
        gs[l] = theirs.astype(jnp.bfloat16)
        gl[l, 1 - y] = theirs[rows - HALO :]
        for half in (1, 0):
            gl_copy(l, half).start()
        pl.when(follows(1 - y))(lambda: halo(l, 1 - y).start())
        mine = tokens(y)
        ext[l, y, HALO:] = mine
        gl[l, y] = mine[rows - HALO :]
        pl.when(follows(y))(lambda: halo(l, y).start())

    def cv_copy(l, q, half):
        here = pl.ds(half * (rows // 2), rows // 2)
        return remote(cvs.at[l, q, here], cvr.at[l, q, here], xsem, cvsem.at[l], sp, peer)

    def conv_rows(l, q, r0):
        tap_cols = pl.ds(pl.multiple_of((tp * 2 + q) * quarter, 128), quarter)
        running = jnp.zeros((HALO, quarter), jnp.float32)
        for k in range(KW):
            at = r0 + k + HALO - (KW - 1)
            running = running + taps_ref[k, l : l + 1, tap_cols] * ext[l, q, at : at + HALO]
        cv[q, r0 : r0 + HALO] = running
        cvs[l, q, r0 : r0 + HALO] = running.astype(jnp.bfloat16)

    def conv(l, q):
        for half in (1, 0):
            for r0 in range(half * rows // 2 + (HALO if half == 0 else 0), (half + 1) * rows // 2, HALO):
                conv_rows(l, q, r0)
            if half == 0:
                pl.when(sp > 0)(lambda: halo_wait(l, q))
                conv_rows(l, q, 0)
            cv_copy(l, q, half).start()

    def take_glu(l):
        landed(gr.at[l], glsem.at[l])
        ext[l, 1 - y, HALO:] = gr[l].astype(jnp.float32)

    def activate(l, between):
        first = jnp.zeros((rows, 1), jnp.float32)
        second = jnp.zeros((rows, 1), jnp.float32)
        for q in range(2):
            value = cv[q]
            first = first + jnp.sum(value, axis=1, keepdims=True)
            second = second + square_sum(value)
        landed(cvr.at[l], cvsem.at[l])
        between()
        for q in range(2):
            value = cvr[l, q].astype(jnp.float32)
            first = first + jnp.sum(value, axis=1, keepdims=True)
            second = second + square_sum(value)
        mean = first / C
        scale = lax.rsqrt(second / C - mean * mean + EPS)
        for half, source in ((tp, None), (peer, cvr)):
            for q in range(2):
                value = cv[q] if source is None else source[l, q].astype(jnp.float32)
                here = pl.ds(pl.multiple_of((half * 2 + q) * quarter, 128), quarter)
                v = (value - mean) * scale * lng_ref[l : l + 1, here] + lnb_ref[l : l + 1, here]
                act[half, :, q * quarter : (q + 1) * quarter] = (v / (1.0 + jnp.exp(-v))).astype(jnp.bfloat16)

    def branch(l, zz):
        total = None
        for cc in range(2):
            weights = jnp.concatenate([ob[l, index(zz, 0, cc)], ob[l, index(zz, 1, cc)]], axis=1)
            partial_sum = jnp.dot(act[cc], weights, preferred_element_type=jnp.float32)
            partial_sum = partial_sum.astype(jnp.bfloat16).astype(jnp.float32)
            total = partial_sum if total is None else total + partial_sum
        return total

    def x1_side(zz):
        return same(x1.at[y, tp, zz], sidesem, x1sem.at[0, zz], side)

    def x1_peer(far, zz):
        block = x1.at[1 - y if far else y, tp, zz]
        return remote(block, block, xsem, x1sem.at[1 + far, zz], sp, peer)

    def x1_diagonal(zz):
        return same(x1.at[y, peer, zz], sidesem, x1sem.at[2, zz], side)

    def step(i):
        return (z + levels + (1 - 2 * (z // half_levels)) * i) % levels

    def project_first(zz):
        o_other_both(zz)
        added = branch(0, zz)
        for part in range(2):
            at = pl.ds(pl.multiple_of((index(zz, part, tp) % (n // 2)) * width, 128), width)
            here = xs[y, zz // half_levels, :, at].astype(jnp.float32)
            x1[y, tp, zz, part] = (
                here + added[:, part * width : (part + 1) * width]).astype(jnp.bfloat16)
        x1_side(zz).start()
        x1_peer(0, zz).start()

    def x2_copy(zz, part):
        return remote(x2.at[zz, part], x2r.at[zz, part], xsem, x2sem, sp, peer)

    def put_last(zz, part, added):
        fresh = (x1[y, tp, zz, part].astype(jnp.float32) + added).astype(jnp.bfloat16)
        x2[zz, part] = fresh
        pl.when(zz // half_levels == peer)(lambda: x2_copy(zz, part).start())
        return square_sum(fresh.astype(jnp.float32))

    def project_last(zz):
        o_other(zz, y)
        o_other(zz, 1 - y)
        added = branch(1, zz)
        return put_last(zz, 0, added[:, :width]) + put_last(zz, 1, added[:, width:])

    def project_end(zz):
        total = None
        for part in (y, 1 - y):
            if total is not None:
                o_across(1, zz)
            o_other(zz, part)
            added = None
            for cc in range(2):
                one = jnp.dot(act[cc], ob[1, index(zz, part, cc)], preferred_element_type=jnp.float32)
                one = one.astype(jnp.bfloat16).astype(jnp.float32)
                added = one if added is None else added + one
            one = put_last(zz, part, added)
            total = one if total is None else total + one
        return total

    def stat_copy():
        return remote(st, rst, tsem.at[0], tsem.at[1], sp, peer)

    landed(vg.at[0 : 2 * LAYERS], isem.at[0])
    pick_rows(0)

    @pl.when(sp == 0)
    def _():
        for l in range(LAYERS):
            for q in range(2):
                ext[l, q, 0:HALO] = jnp.zeros((HALO, quarter), jnp.float32)

    ends = [has_up, has_down, swaps, follows(0), follows(1)]
    pl.semaphore_wait(barrier, 3 + sum(end.astype(jnp.int32) for end in ends))

    for half in range(gives(0)):
        vg_give(0, half).start()
    vg_own(0)
    loads[2].wait()
    x_peer(0).start()
    x_side().start()
    pick_rows(1)
    for half in range(gives(1)):
        vg_give(1, half).start()
    loads[3].wait()
    for l in range(LAYERS):
        pick_columns(l)
    middle = jnp.logical_and(has_up, has_down)
    last = jnp.logical_not(middle)
    near = range(1, levels - 1)
    lower, upper = z < half_levels, z >= half_levels

    for load in loads[4:]:
        load.wait()
    vg_side(0)
    for d in near:
        vg_line(0, d)
        if d == 1:
            x_peer(0).wait_recv()
            normalise_first(y)
            o_swapped(0)
            pl.when(last)(lambda: o_own_line(0, has_up, has_down))
            x_side().wait_recv()
            x_peer(1).start()
    pl.when(middle)(lambda: o_own_line(0, lower, upper))
    o_own_here(0)
    vg_line(0, levels - 1)
    x_peer(1).wait_recv()
    normalise_first(1 - y)
    vg_other(0)
    pl.when(middle)(lambda: o_own_line(0, upper, lower))
    glu(0)

    def o_near(l, *distances):
        for d in distances:
            o_line(l, d)

    pl.when(middle)(lambda: o_near(0, *near))
    vg_own(1)
    vg_side(1)
    conv(0, y)
    pl.when(last)(lambda: o_near(0, 1))
    take_glu(0)
    conv(0, 1 - y)
    o_across(0, step(0))
    pl.when(last)(lambda: o_near(0, *near[1:], levels - 1))
    activate(0, lambda: o_across(0, step(1)))
    project_first(step(0))
    o_across(0, step(2))
    project_first(step(1))
    pl.when(middle)(lambda: vg_line(1, 1))
    for i in range(2, levels):
        if i > 2:
            o_across(0, step(i))
        project_first(step(i))
    pl.when(last)(lambda: vg_line(1, 1))
    for i in range(0, levels, 2):
        x1_peer(0, step(i)).wait_recv()
        x1_peer(0, step(i + 1)).wait_recv()
        x1_diagonal(step(i + 1)).start()
        x1_side(step(i)).wait_recv()
        x1_peer(1, step(i)).start()
        x1_side(step(i + 1)).wait_recv()
    for d in near[1:]:
        vg_line(1, d)
    normalise_next(y)
    o_swapped(1)
    pl.when(last)(lambda: o_own_line(1, has_up, has_down))
    pl.when(middle)(lambda: o_own_line(1, lower, upper))
    o_own_here(1)
    for i in range(levels):
        if i % 2 == 0:
            x1_peer(1, step(i)).wait_recv()
        else:
            x1_diagonal(step(i)).wait_recv()
    normalise_next(1 - y)
    vg_line(1, levels - 1)
    early = jnp.logical_and(last, core == 1)
    late = jnp.logical_and(last, core == 0)
    pl.when(early)(lambda: o_near(1, 1))
    vg_other(1)
    glu(1)

    @pl.when(middle)
    def _():
        o_own_line(1, upper, lower)
        o_near(1, *near)

    conv(1, y)
    pl.when(early)(lambda: o_near(1, *near[1:]))
    pl.when(late)(lambda: o_near(1, 1))
    take_glu(1)
    conv(1, 1 - y)
    o_across(1, step(0))
    pl.when(early)(lambda: o_near(1, levels - 1))
    pl.when(late)(lambda: o_near(1, *near[1:], levels - 1))
    activate(1, lambda: o_across(1, step(1)))
    squares = project_last(step(0))
    for i in range(1, levels - 1):
        o_across(1, step(i + 1)) if i + 1 < levels - 1 else None
        squares = squares + project_last(step(i))
    squares = squares + project_end(step(levels - 1))
    st[...] = jnp.broadcast_to(squares, (rows, 128)).T[0:8]
    stat_copy().start()

    for zz in range(levels):
        @pl.when(z == zz)
        def _():
            for sem, count in ((upsem, zz + 1 if zz < levels - 1 else 0), (downsem, levels - zz if zz > 0 else 0)):
                if count:
                    landed(vg.at[0 : 3 * LAYERS * count], sem)
    landed(vg.at[0 : 2 * n], coresem)
    landed(vg.at[0 : LAYERS + LAYERS * levels + 2 + levels // 2 + levels // 4 + LAYERS // 2], sidesem)
    pl.when(swaps)(lambda: landed(osw, swsem.at[0]))
    for yy in range(2):
        pl.when(follows(yy))(lambda: landed(gl.at[0], hssem.at[yy]))

    stat_copy().wait_recv()
    landed(x2r.at[0:half_levels], x2sem)
    both = st[...] + rst[...]
    total = jnp.concatenate([both] * (128 // 8), axis=0).T[:, 0:1]
    scale = lax.rsqrt(total / D + EPS)
    for i in range(half_levels):
        zz = tp * half_levels + i
        for part in range(2):
            for source, parity in ((x2, tp), (x2r, peer)):
                at = ((i * 2 + part) * 2 + parity) * width
                gain = fg_ref[0:1, pl.ds(pl.multiple_of(tp * cols + at, 128), width)]
                value = source[zz, part].astype(jnp.float32)
                out_ref[:, pl.ds(pl.multiple_of(at, 128), width)] = (value * scale * gain).astype(jnp.bfloat16)
    landed(vg.at[0 : 4 + levels // 2 + levels // 4 + LAYERS + levels // 4], xsem)
    stat_copy().wait_send()


def fused(n, stream, norm_gain, value_weight, gate_weight, conv_taps, ln_gain, ln_bias, out_weight, final_gain):
    rows, cols = stream.shape
    depth, ch = value_weight.shape[0] // LAYERS, value_weight.shape[1]
    width = out_weight.shape[1] // LAYERS
    levels = n // 4
    bf16, f32 = jnp.bfloat16, jnp.float32
    dma = pltpu.SemaphoreType.DMA
    arrays = (stream, norm_gain, value_weight, gate_weight, conv_taps.transpose(1, 0, 2),
              ln_gain, ln_bias, out_weight, final_gain.reshape(1, -1))
    return pl.pallas_call(
        functools.partial(fused_kernel, n),
        out_shape=pltpu.VMEM((rows, cols), bf16),
        in_specs=[pl.BlockSpec(memory_space=pl.ANY)] * 9,
        out_specs=pl.BlockSpec(memory_space=pltpu.VMEM),
        scratch_shapes=[pltpu.VMEM(array.shape, array.dtype) for array in arrays[1:]] + [
            dma((len(arrays) - 1,)),
            pltpu.VMEM((LAYERS * n, depth, ch), bf16),
            pltpu.VMEM((LAYERS, depth, ch), bf16),
            pltpu.VMEM((LAYERS, n, ch, width), bf16),
            pltpu.VMEM((LAYERS, ch, width), bf16),
            pltpu.VMEM((2, 2, rows, cols), bf16),
            pltpu.VMEM((2, 2, levels, 2, rows, width), bf16),
            pltpu.VMEM((levels, 2, rows, width), bf16),
            pltpu.VMEM((levels, 2, rows, width), bf16),
            pltpu.VMEM((2, rows, 2 * cols), bf16),
            pltpu.VMEM((LAYERS, 2, HALO, ch // 2), f32),
            pltpu.VMEM((LAYERS, rows, ch // 2), bf16),
            pltpu.VMEM((LAYERS, rows, ch // 2), bf16),
            pltpu.VMEM((LAYERS, 2, HALO + rows, ch // 2), f32),
            pltpu.VMEM((2, rows, ch // 2), f32),
            pltpu.VMEM((LAYERS, 2, rows, ch // 2), bf16),
            pltpu.VMEM((LAYERS, 2, rows, ch // 2), bf16),
            pltpu.VMEM((2, rows, ch), bf16),
            pltpu.VMEM((8, rows), f32),
            pltpu.VMEM((8, rows), f32),
            dma, dma, dma, dma, dma,
            dma((LAYERS + 1,)),
            dma((LAYERS, n // 2)),
            dma((LAYERS,)),
            dma((n // 2 + n,)),
            dma((levels + n // 2,)),
            dma((1 + LAYERS,)),
            dma((3,)),
            dma((3, levels)),
            dma,
            dma((LAYERS,)),
            dma((LAYERS,)),
            dma((2,)),
            dma((LAYERS, 2)),
            dma((2,)),
        ],
        compiler_params=pltpu.CompilerParams(collective_id=0, has_side_effects=True),
    )(*arrays)


def solution(mesh):
    placed = (P("sp", "tp"), P(), P("sp", "tp"), P("sp", "tp"), P(), P(), P(), P("tp", "sp"), P())
    n, n_tp = mesh.shape["sp"], mesh.shape["tp"]

    def step(*args):
        stream, out_weight = args[0], args[7]
        fits = (n_tp == 2 and n % 8 == 0 and stream.shape[0] == 128 and out_weight.shape[1] == 128 * LAYERS
                and args[2].shape == (128 * LAYERS, 512))
        return fused(n, *args) if fits else local(*args)

    return jax.shard_map(step, mesh=mesh, in_specs=placed, out_specs=P("sp", "tp"), check_vma=False)
```

```python
import functools

import jax
import jax.numpy as jnp
from jax import lax
from jax.experimental import pallas as pl
from jax.experimental.pallas import tpu as pltpu
from jax.sharding import PartitionSpec as P

D = 2048
C = 1024
KW = 31
LAYERS = 2


EPS = 1e-06


def from_behind(value, axis, steps):
    count = lax.axis_size(axis)
    first, last = (max(0, -steps), min(count, count - steps))
    return lax.ppermute(value, axis, [(source, source + steps) for source in range(first, last)])


def valid_conv(extended, tap_table):
    length = extended.shape[0] - (KW - 1)
    running = tap_table[0] * extended[0:length]
    for tap_index in range(1, KW):
        running = running + tap_table[tap_index] * extended[tap_index : tap_index + length]
    return running


def local(
    stream,
    norm_gain,
    value_weight,
    gate_weight,
    conv_taps,
    ln_gain,
    ln_bias,
    out_weight,
    final_gain,
):
    tokens_here = stream.shape[0]
    columns = stream.shape[1]
    channels = value_weight.shape[1]
    rim_rows = KW - 1
    tp_index = lax.axis_index("tp")
    my_taps = lax.dynamic_slice_in_dim(conv_taps, tp_index * channels, channels, 2)
    my_ln_gain = lax.dynamic_slice_in_dim(ln_gain, tp_index * channels, channels, 1)
    my_ln_bias = lax.dynamic_slice_in_dim(ln_bias, tp_index * channels, channels, 1)
    my_final = lax.dynamic_slice_in_dim(final_gain, tp_index * columns, columns, 0)
    value_all, gate_all, out_all = (
        lax.all_gather(value_weight, "sp", axis=0, tiled=True),
        lax.all_gather(gate_weight, "sp", axis=0, tiled=True),
        lax.all_gather(out_weight, "sp", axis=1, tiled=True),
    )
    value_all = value_all.reshape(D, LAYERS, channels)
    gate_all = gate_all.reshape(D, LAYERS, channels)
    out_all = out_all.reshape(channels, D, LAYERS)
    earlier = from_behind(stream[-LAYERS * rim_rows :], "sp", 1)
    current = jnp.concatenate([earlier, stream], axis=0)
    for layer_index in range(LAYERS):
        prefix = (LAYERS - layer_index) * rim_rows
        gathered = lax.all_gather(current, "tp", axis=1, tiled=True)
        gathered32 = gathered.astype(jnp.float32)
        scale = lax.rsqrt(jnp.sum(gathered32 * gathered32, axis=1, keepdims=True) / D + EPS)
        run_normed = (gathered32 * scale * norm_gain[layer_index]).astype(jnp.bfloat16)
        value_proj = jnp.dot(
            run_normed, value_all[:, layer_index], preferred_element_type=jnp.float32
        )
        gate_proj = jnp.dot(
            run_normed, gate_all[:, layer_index], preferred_element_type=jnp.float32
        )
        glu_out = value_proj * jax.nn.sigmoid(gate_proj)
        positions = (
            lax.axis_index("sp") * tokens_here - prefix + lax.iota(jnp.int32, current.shape[0])
        )
        extended = jnp.where((positions >= 0)[:, None], glu_out, 0.0)
        residual = current[rim_rows:].astype(jnp.float32)
        conv_out = valid_conv(extended, my_taps[layer_index])
        first_sums, square_sums = lax.psum(
            (jnp.sum(conv_out, axis=1), jnp.sum(conv_out * conv_out, axis=1)), "tp"
        )
        row_mean = (first_sums / C)[:, None]
        row_var = (square_sums / C)[:, None] - row_mean * row_mean
        run_active = jax.nn.silu(
            (conv_out - row_mean) * lax.rsqrt(row_var + EPS) * my_ln_gain[layer_index]
            + my_ln_bias[layer_index]
        ).astype(jnp.bfloat16)
        partial_value = jnp.dot(
            run_active, out_all[:, :, layer_index], preferred_element_type=jnp.float32
        )
        summed = lax.psum_scatter(
            partial_value.astype(jnp.bfloat16), "tp", scatter_dimension=1, tiled=True
        ).astype(jnp.float32)
        current = (residual + summed).astype(jnp.bfloat16)
    final32 = current.astype(jnp.float32)
    squares = lax.psum(jnp.sum(final32 * final32, axis=1), "tp")
    return (final32 * lax.rsqrt(squares[:, None] / D + EPS) * my_final).astype(jnp.bfloat16)


MESH = pl.DeviceIdType.MESH
HALO = 32


def fused_kernel(
    n, x_in, ng_in, v_in, g_in, taps_in, lng_in, lnb_in, o_in, fg_in, out_ref,
    ng_ref, v_ref, g_ref, taps_ref, lng_ref, lnb_ref, o_ref, fg_ref, isem,
    vg, gv, ob, osw, xs, x1, x2, x2r, nb, gl, gs, gr, ext, cv, cvs, cvr, act, st, rst,
    upsem, downsem, sidesem, coresem, xsem, gvsem, vgsem, vcsem, osem, ocsem, swsem, xrsem, x1sem, x2sem, cvsem, glsem, hssem, hsem, tsem,
):
    levels = n // 4
    half_levels = levels // 2
    sp = lax.axis_index("sp")
    tp = lax.axis_index("tp")
    z, y, core = sp // 4, (sp // 2) % 2, sp % 2
    peer = 1 - tp
    rows, cols = xs.shape[2], xs.shape[3]
    depth, quarter = vg.shape[1], vg.shape[2] // 2
    width = ob.shape[3]
    has_up, has_down = z < levels - 1, z > 0
    swaps = tp + core == 1
    middle = jnp.logical_and(has_up, has_down)
    last = jnp.logical_not(middle)
    near = range(1, levels - 1)
    lower, upper = z < half_levels, z >= half_levels
    side, twin = sp + 2 - 4 * y, sp + 1 - 2 * core

    def index(zz, yy, cc):
        return (zz * 2 + yy) * 2 + cc

    def landed(block, sem):
        pltpu.make_async_copy(block, block, sem).wait()

    def remote(src, dst, send, recv, to_sp, to_tp):
        return pltpu.make_async_remote_copy(
            src_ref=src, dst_ref=dst, send_sem=send, recv_sem=recv,
            device_id={"sp": to_sp, "tp": to_tp}, device_id_type=MESH)

    def same(ref, send, recv, to_sp):
        return remote(ref, ref, send, recv, to_sp, tp)

    barrier = pltpu.get_barrier_semaphore()

    def greet(to_sp, to_tp):
        pl.semaphore_signal(barrier, inc=1, device_id={"sp": to_sp, "tp": to_tp}, device_id_type=MESH)

    greet(side, tp)
    greet(twin, tp)
    greet(sp, peer)
    pl.when(has_up)(lambda: greet(sp + 4, tp))
    pl.when(has_down)(lambda: greet(sp - 4, tp))
    pl.when(swaps)(lambda: greet(twin, peer))
    before = sp - 1

    @pl.when(sp > 0)
    def _():
        for yy in range(2):
            greet(index(before // 4, yy, before % 2), tp)

    loads = [
        pltpu.make_async_copy(source, to, isem.at[max(i - 1, 0)])
        for i, (source, to) in enumerate((
            (v_in, v_ref), (g_in, g_ref), (x_in, xs.at[y, tp]), (o_in, o_ref), (ng_in, ng_ref),
            (taps_in, taps_ref), (lng_in, lng_ref), (lnb_in, lnb_ref), (fg_in, fg_ref)))
    ]
    for load in loads:
        load.start()

    def follows(yy):
        return index(z, yy, core) + 1 < n

    def vg_copy(l, src, send, to_sp):
        return same(vg.at[l * n + src], send, vgsem.at[l, src // 2], to_sp)

    def gives(l):
        return 2 if l == 0 else 1

    def vg_rows(l, half):
        return pl.ds(half * (depth // gives(l)), depth // gives(l))

    def vg_give(l, half):
        here = vg_rows(l, half)
        return remote(
            gv.at[l, here], vg.at[l * n + sp, here], sidesem, gvsem.at[half if l == 0 else l + 1], side, tp)

    def vg_take(l, src):
        vg_copy(l, src, coresem, twin).wait_recv()

    def vg_up(l, src):
        pl.when(has_up)(lambda: vg_copy(l, src, upsem, sp + 4).start())

    def vg_down(l, src):
        pl.when(has_down)(lambda: vg_copy(l, src, downsem, sp - 4).start())

    def vg_core(l, src):
        same(vg.at[l * n + src], coresem, vcsem.at[l], twin).start()

    def vg_own(l):
        vg_up(l, sp)
        vg_down(l, sp)
        vg_core(l, sp)

    def vg_side(l):
        src = index(z, 1 - y, core)
        for half in range(gives(l)):
            vg_give(l, half).wait_recv()
            block = vg.at[l * n + src, vg_rows(l, half)]
            pl.when(has_up)(lambda: same(block, upsem, vgsem.at[l, src // 2], sp + 4).start())
            pl.when(has_down)(lambda: same(block, downsem, vgsem.at[l, src // 2], sp - 4).start())
        vg_core(l, src)

    def vg_line(l, d):
        def one(zz, onward):
            for yy in (y, 1 - y):
                src = index(zz, yy, core)
                vg_take(l, src)
                onward(l, src)
                vg_core(l, src)

        pl.when(z - d >= 0)(lambda: one(z - d, vg_up))
        pl.when(z + d < levels)(lambda: one(z + d, vg_down))

    def vg_other(l):
        landed(vg.at[0 : n // 2], vcsem.at[l])

    def halves(l):
        return range(2 if l == LAYERS - 1 else 1)

    def o_block(l, src, half):
        size = ob.shape[2] // len(halves(l))
        return ob.at[l, src, pl.ds(half * size, size)]

    def o_copy(l, src, half, send, to_sp):
        at = src // 2 if l == 0 else n // 2 + src // 2 * 2 + half
        return same(o_block(l, src, half), send, osem.at[at], to_sp)

    def o_core(l, src, half):
        at = src // 4 if l == 0 else levels + src // 2
        same(o_block(l, src, half), coresem, ocsem.at[at], twin).start()

    def o_swap(l):
        return remote(osw.at[l], ob.at[l, twin], swsem.at[0], swsem.at[1 + l], twin, peer)

    def o_take(l, src, half):
        o_copy(l, src, half, sidesem, side).wait_recv()

    def o_up(l, src, half):
        pl.when(has_up)(lambda: o_copy(l, src, half, upsem, sp + 4).start())

    def o_down(l, src, half):
        pl.when(has_down)(lambda: o_copy(l, src, half, downsem, sp - 4).start())

    def o_here(l, src, half):
        o_copy(l, src, half, sidesem, side).start()
        o_core(l, src, half)

    def o_swapped(l):
        pl.when(swaps)(lambda: o_swap(l).wait_recv())

    def o_own_line(l, up, down):
        for half in halves(l):
            pl.when(up)(lambda: o_up(l, sp, half))
            pl.when(down)(lambda: o_down(l, sp, half))

    def o_own_here(l):
        for half in halves(l):
            o_here(l, sp, half)

    def o_line(l, d):
        def one(zz, onward):
            src = index(zz, y, core)
            for half in halves(l):
                o_take(l, src, half)
                onward(l, src, half)
                if l == LAYERS - 1 and d == 1:
                    pl.when(middle)(lambda: o_copy(l, src, half, sidesem, side).start())
                    o_core(l, src, half)
                else:
                    o_here(l, src, half)

        pl.when(z - d >= 0)(lambda: one(z - d, o_up))
        pl.when(z + d < levels)(lambda: one(z + d, o_down))

    def o_across(l, zz):
        src = index(zz, 1 - y, core)
        for half in halves(l):
            o_take(l, src, half)
            o_core(l, src, half)

    def o_across_end(l):
        src = index(z, 1 - y, core)
        for half in halves(l):
            pl.when(z == 1)(lambda: o_copy(l, src, half, downsem, sp - 4).start())
            pl.when(z == levels - 2)(lambda: o_copy(l, src, half, upsem, sp + 4).start())

    def o_other_both(zz):
        landed(ob.at[0, 0:2], ocsem.at[zz])

    def o_other(zz, yy):
        landed(ob.at[0, 0], ocsem.at[levels + zz * 2 + yy])

    lo = lax.broadcasted_iota(jnp.int32, (depth, LAYERS * depth), 0)
    hi = lax.broadcasted_iota(jnp.int32, (depth, LAYERS * depth), 1)
    clo = lax.broadcasted_iota(jnp.int32, (LAYERS * width, width), 1)
    chi = lax.broadcasted_iota(jnp.int32, (LAYERS * width, width), 0)

    def pick_rows(l):
        pick = (hi == LAYERS * lo + l).astype(jnp.float32).astype(jnp.bfloat16)
        for yy, keep in ((1 - y, False), (y, True)):
            here = pl.ds(pl.multiple_of(yy * quarter, 128), quarter)
            for kind, ref in enumerate((v_ref, g_ref)):
                picked = jnp.dot(pick, ref[:, here], preferred_element_type=jnp.float32).astype(jnp.bfloat16)
                at = kind * quarter
                if keep:
                    vg[l * n + sp, :, at : at + quarter] = picked
                else:
                    gv[l, :, at : at + quarter] = picked

    def pick_columns(l):
        pick = (chi == LAYERS * clo + l).astype(jnp.float32).astype(jnp.bfloat16)
        picked = jnp.dot(o_ref[...], pick, preferred_element_type=jnp.float32).astype(jnp.bfloat16)

        @pl.when(swaps)
        def _():
            osw[l] = picked
            o_swap(l).start()

        @pl.when(jnp.logical_not(swaps))
        def _():
            ob[l, sp] = picked

    def x_side():
        return same(xs.at[y, tp], sidesem, xrsem.at[0], side)

    def x_peer(far):
        block = xs.at[1 - y if far else y, tp]
        return remote(block, block, xsem, xrsem.at[1 + far], sp, peer)

    def square_sum(value):
        return jnp.sum(value * value, axis=1, keepdims=True)

    def normalise_first(yy):
        total = jnp.zeros((rows, 1), jnp.float32)
        for half in range(2):
            total = total + square_sum(xs[yy, half].astype(jnp.float32))
        scale = lax.rsqrt(total / D + EPS)
        for half in range(2):
            gain = ng_ref[0:1, half * cols : (half + 1) * cols]
            nb[yy, :, half * cols : (half + 1) * cols] = (
                xs[yy, half].astype(jnp.float32) * scale * gain).astype(jnp.bfloat16)

    def normalise_next(yy):
        total = jnp.zeros((rows, 1), jnp.float32)
        for half in range(2):
            for zz in range(levels):
                for part in range(2):
                    total = total + square_sum(x1[yy, half, zz, part].astype(jnp.float32))
        scale = lax.rsqrt(total / D + EPS)
        for half in range(2):
            for zz in range(levels):
                for part in range(2):
                    at = index(zz, part, half) * width
                    value = x1[yy, half, zz, part].astype(jnp.float32)
                    nb[yy, :, at : at + width] = (
                        value * scale * ng_ref[1:2, at : at + width]).astype(jnp.bfloat16)

    def gl_copy(l, half):
        here = pl.ds(half * (rows // 2), rows // 2)
        return remote(gs.at[l, here], gr.at[l, here], sidesem, glsem.at[l], side, tp)

    def halo(l, yy):
        return remote(
            gl.at[l, yy], ext.at[l, y, pl.ds(0, HALO)],
            hssem.at[yy], hsem.at[l, y], index(z, yy, core) + 1, tp)

    def halo_wait(l, q):
        remote(
            gl.at[l, 0], ext.at[l, q, pl.ds(0, HALO)],
            hssem.at[0], hsem.at[l, q], side, tp).wait_recv()

    def glu(l):
        weights = vg[l * n : (l + 1) * n].reshape(n * depth, 2 * quarter)

        def tokens(yy):
            both = jnp.dot(nb[yy], weights, preferred_element_type=jnp.float32)
            return both[:, :quarter] * jax.nn.sigmoid(both[:, quarter:])

        theirs = tokens(1 - y)
        gs[l] = theirs.astype(jnp.bfloat16)
        gl[l, 1 - y] = theirs[rows - HALO :]
        for half in (1, 0):
            gl_copy(l, half).start()
        pl.when(follows(1 - y))(lambda: halo(l, 1 - y).start())
        mine = tokens(y)
        ext[l, y, HALO:] = mine
        gl[l, y] = mine[rows - HALO :]
        pl.when(follows(y))(lambda: halo(l, y).start())

    def cv_copy(l, q, half):
        here = pl.ds(half * (rows // 2), rows // 2)
        return remote(cvs.at[l, q, here], cvr.at[l, q, here], xsem, cvsem.at[l], sp, peer)

    def conv_rows(l, q, r0):
        tap_cols = pl.ds(pl.multiple_of((tp * 2 + q) * quarter, 128), quarter)
        running = jnp.zeros((HALO, quarter), jnp.float32)
        for k in range(KW):
            at = r0 + k + HALO - (KW - 1)
            running = running + taps_ref[k, l : l + 1, tap_cols] * ext[l, q, at : at + HALO]
        cv[q, r0 : r0 + HALO] = running
        cvs[l, q, r0 : r0 + HALO] = running.astype(jnp.bfloat16)

    def conv(l, q):
        for half in (1, 0):
            for r0 in range(half * rows // 2 + (HALO if half == 0 else 0), (half + 1) * rows // 2, HALO):
                conv_rows(l, q, r0)
            if half == 0:
                pl.when(sp > 0)(lambda: halo_wait(l, q))
                conv_rows(l, q, 0)
            cv_copy(l, q, half).start()

    def take_glu(l):
        landed(gr.at[l], glsem.at[l])
        ext[l, 1 - y, HALO:] = gr[l].astype(jnp.float32)

    def activate(l, between):
        first = jnp.zeros((rows, 1), jnp.float32)
        second = jnp.zeros((rows, 1), jnp.float32)
        for q in range(2):
            value = cv[q]
            first = first + jnp.sum(value, axis=1, keepdims=True)
            second = second + square_sum(value)
        landed(cvr.at[l], cvsem.at[l])
        between()
        for q in range(2):
            value = cvr[l, q].astype(jnp.float32)
            first = first + jnp.sum(value, axis=1, keepdims=True)
            second = second + square_sum(value)
        mean = first / C
        scale = lax.rsqrt(second / C - mean * mean + EPS)
        for half, source in ((tp, None), (peer, cvr)):
            for q in range(2):
                value = cv[q] if source is None else source[l, q].astype(jnp.float32)
                here = pl.ds(pl.multiple_of((half * 2 + q) * quarter, 128), quarter)
                v = (value - mean) * scale * lng_ref[l : l + 1, here] + lnb_ref[l : l + 1, here]
                act[half, :, q * quarter : (q + 1) * quarter] = (v / (1.0 + jnp.exp(-v))).astype(jnp.bfloat16)

    def branch(l, zz):
        total = None
        for cc in range(2):
            weights = jnp.concatenate([ob[l, index(zz, 0, cc)], ob[l, index(zz, 1, cc)]], axis=1)
            partial_sum = jnp.dot(act[cc], weights, preferred_element_type=jnp.float32)
            partial_sum = partial_sum.astype(jnp.bfloat16).astype(jnp.float32)
            total = partial_sum if total is None else total + partial_sum
        return total

    def x1_side(zz):
        return same(x1.at[y, tp, zz], sidesem, x1sem.at[0, zz], side)

    def x1_peer(far, zz):
        block = x1.at[1 - y if far else y, tp, zz]
        return remote(block, block, xsem, x1sem.at[1 + far, zz], sp, peer)

    def x1_diagonal(zz):
        return same(x1.at[y, peer, zz], sidesem, x1sem.at[2, zz], side)

    def step(i):
        return (z + levels + (1 - 2 * (z // half_levels)) * i) % levels

    def project_first(zz):
        o_other_both(zz)
        added = branch(0, zz)
        for part in range(2):
            at = pl.ds(pl.multiple_of((index(zz, part, tp) % (n // 2)) * width, 128), width)
            here = xs[y, zz // half_levels, :, at].astype(jnp.float32)
            x1[y, tp, zz, part] = (
                here + added[:, part * width : (part + 1) * width]).astype(jnp.bfloat16)
        x1_side(zz).start()
        x1_peer(0, zz).start()

    def x2_copy(zz, part):
        return remote(x2.at[zz, part], x2r.at[zz, part], xsem, x2sem, sp, peer)

    def put_last(zz, part, added):
        fresh = (x1[y, tp, zz, part].astype(jnp.float32) + added).astype(jnp.bfloat16)
        x2[zz, part] = fresh
        pl.when(zz // half_levels == peer)(lambda: x2_copy(zz, part).start())
        return square_sum(fresh.astype(jnp.float32))

    def project_last(zz):
        o_other(zz, y)
        o_other(zz, 1 - y)
        added = branch(1, zz)
        return put_last(zz, 0, added[:, :width]) + put_last(zz, 1, added[:, width:])

    def project_part(zz, part):
        o_other(zz, part)
        added = None
        for cc in range(2):
            one = jnp.dot(act[cc], ob[1, index(zz, part, cc)], preferred_element_type=jnp.float32)
            one = one.astype(jnp.bfloat16).astype(jnp.float32)
            added = one if added is None else added + one
        return put_last(zz, part, added)

    def stat_copy():
        return remote(st, rst, tsem.at[0], tsem.at[1], sp, peer)

    landed(vg.at[0 : 2 * LAYERS], isem.at[0])
    pick_rows(0)

    @pl.when(sp == 0)
    def _():
        for l in range(LAYERS):
            for q in range(2):
                ext[l, q, 0:HALO] = jnp.zeros((HALO, quarter), jnp.float32)

    ends = [has_up, has_down, swaps, follows(0), follows(1)]
    pl.semaphore_wait(barrier, 3 + sum(end.astype(jnp.int32) for end in ends))

    for half in range(gives(0)):
        vg_give(0, half).start()
    vg_own(0)
    loads[2].wait()
    x_peer(0).start()
    x_side().start()
    pick_rows(1)
    for half in range(gives(1)):
        vg_give(1, half).start()
    loads[3].wait()
    for l in range(LAYERS):
        pick_columns(l)
    for load in loads[4:]:
        load.wait()
    vg_side(0)
    for d in near:
        vg_line(0, d)
        if d == 1:
            x_peer(0).wait_recv()
            normalise_first(y)
            o_swapped(0)
            pl.when(last)(lambda: o_own_line(0, has_up, has_down))
            x_side().wait_recv()
            x_peer(1).start()
    pl.when(middle)(lambda: o_own_line(0, lower, upper))
    o_own_here(0)
    vg_line(0, levels - 1)
    x_peer(1).wait_recv()
    normalise_first(1 - y)
    vg_other(0)
    pl.when(middle)(lambda: o_own_line(0, upper, lower))
    glu(0)

    def o_near(l, *distances):
        for d in distances:
            o_line(l, d)

    pl.when(middle)(lambda: o_near(0, *near))
    vg_own(1)
    vg_side(1)
    conv(0, y)
    pl.when(last)(lambda: o_near(0, 1))
    take_glu(0)
    conv(0, 1 - y)
    o_across(0, step(0))
    pl.when(last)(lambda: o_near(0, *near[1:], levels - 1))
    activate(0, lambda: o_across(0, step(1)))
    project_first(step(0))
    o_across(0, step(2))
    project_first(step(1))
    pl.when(middle)(lambda: vg_line(1, 1))
    for i in range(2, levels):
        if i > 2:
            o_across(0, step(i))
        project_first(step(i))
    pl.when(last)(lambda: vg_line(1, 1))
    for i in range(0, levels, 2):
        x1_peer(0, step(i)).wait_recv()
        x1_peer(0, step(i + 1)).wait_recv()
        x1_diagonal(step(i + 1)).start()
        x1_side(step(i)).wait_recv()
        x1_peer(1, step(i)).start()
        x1_side(step(i + 1)).wait_recv()
    for d in near[1:]:
        vg_line(1, d)
    normalise_next(y)
    o_swapped(1)
    pl.when(last)(lambda: o_own_line(1, has_up, has_down))
    pl.when(middle)(lambda: o_own_line(1, lower, upper))
    o_own_here(1)
    for i in range(levels):
        if i % 2 == 0:
            x1_peer(1, step(i)).wait_recv()
        else:
            x1_diagonal(step(i)).wait_recv()
    normalise_next(1 - y)
    vg_line(1, levels - 1)
    early = jnp.logical_and(last, core == 1)
    late = jnp.logical_and(last, core == 0)
    pl.when(early)(lambda: o_near(1, 1))
    vg_other(1)
    glu(1)

    @pl.when(middle)
    def _():
        o_own_line(1, upper, lower)
        o_near(1, *near)
        o_across(1, z)
        o_across_end(1)

    conv(1, y)
    pl.when(early)(lambda: o_near(1, *near[1:]))
    pl.when(late)(lambda: o_near(1, 1))
    take_glu(1)
    conv(1, 1 - y)
    pl.when(last)(lambda: o_across(1, z))
    pl.when(early)(lambda: o_near(1, levels - 1))
    pl.when(late)(lambda: o_near(1, *near[1:], levels - 1))
    at_end = last.astype(jnp.int32)

    def order(i):
        if i == 0:
            return step(0)
        return step(i + at_end if i < levels - 1 else levels - 1 - at_end * (levels - 2))

    activate(1, lambda: None)
    squares = project_last(order(0))

    @pl.when(core == 1)
    def _():
        for i in range(1, levels):
            o_across(1, order(i))

    squares = squares + project_part(order(levels - 1), y)
    for i in near:
        pl.when(core == 0)(lambda: o_across(1, order(i)))
        squares = squares + project_last(order(i))
    pl.when(core == 0)(lambda: o_across(1, order(levels - 1)))
    squares = squares + project_part(order(levels - 1), 1 - y)
    st[...] = jnp.broadcast_to(squares, (rows, 128)).T[0:8]
    stat_copy().start()

    for zz in range(levels):
        @pl.when(z == zz)
        def _():
            for sem, count in ((upsem, zz + 1 if zz < levels - 1 else 0), (downsem, levels - zz if zz > 0 else 0)):
                extra = (zz == levels - 2) if sem is upsem else (zz == 1)
                if count:
                    landed(vg.at[0 : 3 * LAYERS * count + extra], sem)
    landed(vg.at[0 : 2 * n], coresem)
    count = LAYERS + LAYERS * levels + 2 + levels // 2 + levels // 4 + LAYERS // 2
    pl.when(middle)(lambda: landed(vg.at[0:count], sidesem))
    pl.when(last)(lambda: landed(vg.at[0 : count - 1], sidesem))
    pl.when(swaps)(lambda: landed(osw, swsem.at[0]))
    for yy in range(2):
        pl.when(follows(yy))(lambda: landed(gl.at[0], hssem.at[yy]))

    stat_copy().wait_recv()
    landed(x2r.at[0:half_levels], x2sem)
    both = st[...] + rst[...]
    total = jnp.concatenate([both] * (128 // 8), axis=0).T[:, 0:1]
    scale = lax.rsqrt(total / D + EPS)
    for i in range(half_levels):
        zz = tp * half_levels + i
        for part in range(2):
            for source, parity in ((x2, tp), (x2r, peer)):
                at = ((i * 2 + part) * 2 + parity) * width
                gain = fg_ref[0:1, pl.ds(pl.multiple_of(tp * cols + at, 128), width)]
                value = source[zz, part].astype(jnp.float32)
                out_ref[:, pl.ds(pl.multiple_of(at, 128), width)] = (value * scale * gain).astype(jnp.bfloat16)
    landed(vg.at[0 : 4 + levels // 2 + levels // 4 + LAYERS + levels // 4], xsem)
    stat_copy().wait_send()


def fused(n, stream, norm_gain, value_weight, gate_weight, conv_taps, ln_gain, ln_bias, out_weight, final_gain):
    rows, cols = stream.shape
    depth, ch = value_weight.shape[0] // LAYERS, value_weight.shape[1]
    width = out_weight.shape[1] // LAYERS
    levels = n // 4
    bf16, f32 = jnp.bfloat16, jnp.float32
    dma = pltpu.SemaphoreType.DMA
    arrays = (stream, norm_gain, value_weight, gate_weight, conv_taps.transpose(1, 0, 2),
              ln_gain, ln_bias, out_weight, final_gain.reshape(1, -1))
    return pl.pallas_call(
        functools.partial(fused_kernel, n),
        out_shape=pltpu.VMEM((rows, cols), bf16),
        in_specs=[pl.BlockSpec(memory_space=pl.ANY)] * 9,
        out_specs=pl.BlockSpec(memory_space=pltpu.VMEM),
        scratch_shapes=[pltpu.VMEM(array.shape, array.dtype) for array in arrays[1:]] + [
            dma((len(arrays) - 1,)),
            pltpu.VMEM((LAYERS * n, depth, ch), bf16),
            pltpu.VMEM((LAYERS, depth, ch), bf16),
            pltpu.VMEM((LAYERS, n, ch, width), bf16),
            pltpu.VMEM((LAYERS, ch, width), bf16),
            pltpu.VMEM((2, 2, rows, cols), bf16),
            pltpu.VMEM((2, 2, levels, 2, rows, width), bf16),
            pltpu.VMEM((levels, 2, rows, width), bf16),
            pltpu.VMEM((levels, 2, rows, width), bf16),
            pltpu.VMEM((2, rows, 2 * cols), bf16),
            pltpu.VMEM((LAYERS, 2, HALO, ch // 2), f32),
            pltpu.VMEM((LAYERS, rows, ch // 2), bf16),
            pltpu.VMEM((LAYERS, rows, ch // 2), bf16),
            pltpu.VMEM((LAYERS, 2, HALO + rows, ch // 2), f32),
            pltpu.VMEM((2, rows, ch // 2), f32),
            pltpu.VMEM((LAYERS, 2, rows, ch // 2), bf16),
            pltpu.VMEM((LAYERS, 2, rows, ch // 2), bf16),
            pltpu.VMEM((2, rows, ch), bf16),
            pltpu.VMEM((8, rows), f32),
            pltpu.VMEM((8, rows), f32),
            dma, dma, dma, dma, dma,
            dma((LAYERS + 1,)),
            dma((LAYERS, n // 2)),
            dma((LAYERS,)),
            dma((n // 2 + n,)),
            dma((levels + n // 2,)),
            dma((1 + LAYERS,)),
            dma((3,)),
            dma((3, levels)),
            dma,
            dma((LAYERS,)),
            dma((LAYERS,)),
            dma((2,)),
            dma((LAYERS, 2)),
            dma((2,)),
        ],
        compiler_params=pltpu.CompilerParams(collective_id=0, has_side_effects=True),
    )(*arrays)


def solution(mesh):
    placed = (P("sp", "tp"), P(), P("sp", "tp"), P("sp", "tp"), P(), P(), P(), P("tp", "sp"), P())
    n, n_tp = mesh.shape["sp"], mesh.shape["tp"]

    def step(*args):
        stream, out_weight = args[0], args[7]
        fits = (n_tp == 2 and n % 8 == 0 and n > 8 and stream.shape[0] == 128 and out_weight.shape[1] == 128 * LAYERS
                and args[2].shape == (128 * LAYERS, 512))
        return fused(n, *args) if fits else local(*args)

    return jax.shard_map(step, mesh=mesh, in_specs=placed, out_specs=P("sp", "tp"), check_vma=False)
```

```python
import functools

import jax
import jax.numpy as jnp
from jax import lax
from jax.experimental import pallas as pl
from jax.experimental.pallas import tpu as pltpu
from jax.sharding import PartitionSpec as P

D = 2048
C = 1024
KW = 31
LAYERS = 2


EPS = 1e-06


def from_behind(value, axis, steps):
    count = lax.axis_size(axis)
    first, last = (max(0, -steps), min(count, count - steps))
    return lax.ppermute(value, axis, [(source, source + steps) for source in range(first, last)])


def valid_conv(extended, tap_table):
    length = extended.shape[0] - (KW - 1)
    running = tap_table[0] * extended[0:length]
    for tap_index in range(1, KW):
        running = running + tap_table[tap_index] * extended[tap_index : tap_index + length]
    return running


def local(
    stream,
    norm_gain,
    value_weight,
    gate_weight,
    conv_taps,
    ln_gain,
    ln_bias,
    out_weight,
    final_gain,
):
    tokens_here = stream.shape[0]
    columns = stream.shape[1]
    channels = value_weight.shape[1]
    rim_rows = KW - 1
    tp_index = lax.axis_index("tp")
    my_taps = lax.dynamic_slice_in_dim(conv_taps, tp_index * channels, channels, 2)
    my_ln_gain = lax.dynamic_slice_in_dim(ln_gain, tp_index * channels, channels, 1)
    my_ln_bias = lax.dynamic_slice_in_dim(ln_bias, tp_index * channels, channels, 1)
    my_final = lax.dynamic_slice_in_dim(final_gain, tp_index * columns, columns, 0)
    value_all, gate_all, out_all = (
        lax.all_gather(value_weight, "sp", axis=0, tiled=True),
        lax.all_gather(gate_weight, "sp", axis=0, tiled=True),
        lax.all_gather(out_weight, "sp", axis=1, tiled=True),
    )
    value_all = value_all.reshape(D, LAYERS, channels)
    gate_all = gate_all.reshape(D, LAYERS, channels)
    out_all = out_all.reshape(channels, D, LAYERS)
    earlier = from_behind(stream[-LAYERS * rim_rows :], "sp", 1)
    current = jnp.concatenate([earlier, stream], axis=0)
    for layer_index in range(LAYERS):
        prefix = (LAYERS - layer_index) * rim_rows
        gathered = lax.all_gather(current, "tp", axis=1, tiled=True)
        gathered32 = gathered.astype(jnp.float32)
        scale = lax.rsqrt(jnp.sum(gathered32 * gathered32, axis=1, keepdims=True) / D + EPS)
        run_normed = (gathered32 * scale * norm_gain[layer_index]).astype(jnp.bfloat16)
        value_proj = jnp.dot(
            run_normed, value_all[:, layer_index], preferred_element_type=jnp.float32
        )
        gate_proj = jnp.dot(
            run_normed, gate_all[:, layer_index], preferred_element_type=jnp.float32
        )
        glu_out = value_proj * jax.nn.sigmoid(gate_proj)
        positions = (
            lax.axis_index("sp") * tokens_here - prefix + lax.iota(jnp.int32, current.shape[0])
        )
        extended = jnp.where((positions >= 0)[:, None], glu_out, 0.0)
        residual = current[rim_rows:].astype(jnp.float32)
        conv_out = valid_conv(extended, my_taps[layer_index])
        first_sums, square_sums = lax.psum(
            (jnp.sum(conv_out, axis=1), jnp.sum(conv_out * conv_out, axis=1)), "tp"
        )
        row_mean = (first_sums / C)[:, None]
        row_var = (square_sums / C)[:, None] - row_mean * row_mean
        run_active = jax.nn.silu(
            (conv_out - row_mean) * lax.rsqrt(row_var + EPS) * my_ln_gain[layer_index]
            + my_ln_bias[layer_index]
        ).astype(jnp.bfloat16)
        partial_value = jnp.dot(
            run_active, out_all[:, :, layer_index], preferred_element_type=jnp.float32
        )
        summed = lax.psum_scatter(
            partial_value.astype(jnp.bfloat16), "tp", scatter_dimension=1, tiled=True
        ).astype(jnp.float32)
        current = (residual + summed).astype(jnp.bfloat16)
    final32 = current.astype(jnp.float32)
    squares = lax.psum(jnp.sum(final32 * final32, axis=1), "tp")
    return (final32 * lax.rsqrt(squares[:, None] / D + EPS) * my_final).astype(jnp.bfloat16)


MESH = pl.DeviceIdType.MESH
HALO = 32


def fused_kernel(
    n, x_in, ng_in, v_in, g_in, taps_in, lng_in, lnb_in, o_in, fg_in, out_ref,
    ng_ref, v_ref, g_ref, taps_ref, lng_ref, lnb_ref, o_ref, fg_ref, isem,
    vg, gv, ob, osw, xs, x1, x2, x2r, nb, gl, gs, gr, ext, cv, cvs, cvr, act, st, rst,
    upsem, downsem, sidesem, coresem, xsem, gvsem, vgsem, vcsem, osem, ocsem, swsem, xrsem, x1sem, x2sem, cvsem, glsem, hssem, hsem, tsem,
):
    levels = n // 4
    half_levels = levels // 2
    sp = lax.axis_index("sp")
    tp = lax.axis_index("tp")
    z, y, core = sp // 4, (sp // 2) % 2, sp % 2
    peer = 1 - tp
    rows, cols = xs.shape[2], xs.shape[3]
    depth, quarter = vg.shape[1], vg.shape[2] // 2
    width = ob.shape[3]
    has_up, has_down = z < levels - 1, z > 0
    swaps = tp + core == 1
    middle = jnp.logical_and(has_up, has_down)
    last = jnp.logical_not(middle)
    near = range(1, levels - 1)
    lower, upper = z < half_levels, z >= half_levels
    side, twin = sp + 2 - 4 * y, sp + 1 - 2 * core

    def index(zz, yy, cc):
        return (zz * 2 + yy) * 2 + cc

    def landed(block, sem):
        pltpu.make_async_copy(block, block, sem).wait()

    def remote(src, dst, send, recv, to_sp, to_tp):
        return pltpu.make_async_remote_copy(
            src_ref=src, dst_ref=dst, send_sem=send, recv_sem=recv,
            device_id={"sp": to_sp, "tp": to_tp}, device_id_type=MESH)

    def same(ref, send, recv, to_sp):
        return remote(ref, ref, send, recv, to_sp, tp)

    barrier = pltpu.get_barrier_semaphore()

    def greet(to_sp, to_tp):
        pl.semaphore_signal(barrier, inc=1, device_id={"sp": to_sp, "tp": to_tp}, device_id_type=MESH)

    greet(side, tp)
    greet(twin, tp)
    greet(sp, peer)
    pl.when(has_up)(lambda: greet(sp + 4, tp))
    pl.when(has_down)(lambda: greet(sp - 4, tp))
    pl.when(swaps)(lambda: greet(twin, peer))
    before = sp - 1

    @pl.when(sp > 0)
    def _():
        for yy in range(2):
            greet(index(before // 4, yy, before % 2), tp)

    loads = [
        pltpu.make_async_copy(source, to, isem.at[max(i - 1, 0)])
        for i, (source, to) in enumerate((
            (v_in, v_ref), (g_in, g_ref), (x_in, xs.at[y, tp]), (o_in, o_ref), (ng_in, ng_ref),
            (taps_in, taps_ref), (lng_in, lng_ref), (lnb_in, lnb_ref), (fg_in, fg_ref)))
    ]
    for load in loads:
        load.start()

    def follows(yy):
        return index(z, yy, core) + 1 < n

    def vg_copy(l, src, send, to_sp):
        return same(vg.at[l * n + src], send, vgsem.at[l, src // 2], to_sp)

    def gives(l):
        return 2 if l == 0 else 1

    def vg_rows(l, half):
        return pl.ds(half * (depth // gives(l)), depth // gives(l))

    def vg_give(l, half):
        here = vg_rows(l, half)
        return remote(
            gv.at[l, here], vg.at[l * n + sp, here], sidesem, gvsem.at[half if l == 0 else l + 1], side, tp)

    def vg_take(l, src):
        vg_copy(l, src, coresem, twin).wait_recv()

    def vg_up(l, src):
        pl.when(has_up)(lambda: vg_copy(l, src, upsem, sp + 4).start())

    def vg_down(l, src):
        pl.when(has_down)(lambda: vg_copy(l, src, downsem, sp - 4).start())

    def vg_core(l, src):
        same(vg.at[l * n + src], coresem, vcsem.at[l], twin).start()

    def vg_own(l):
        vg_up(l, sp)
        vg_down(l, sp)
        vg_core(l, sp)

    def vg_side(l):
        src = index(z, 1 - y, core)
        for half in range(gives(l)):
            vg_give(l, half).wait_recv()
            block = vg.at[l * n + src, vg_rows(l, half)]
            pl.when(has_up)(lambda: same(block, upsem, vgsem.at[l, src // 2], sp + 4).start())
            pl.when(has_down)(lambda: same(block, downsem, vgsem.at[l, src // 2], sp - 4).start())
        vg_core(l, src)

    def vg_line(l, d):
        def one(zz, onward):
            for yy in (y, 1 - y):
                src = index(zz, yy, core)
                vg_take(l, src)
                onward(l, src)
                vg_core(l, src)

        pl.when(z - d >= 0)(lambda: one(z - d, vg_up))
        pl.when(z + d < levels)(lambda: one(z + d, vg_down))

    def vg_other(l):
        landed(vg.at[0 : n // 2], vcsem.at[l])

    def halves(l):
        return range(2 if l == LAYERS - 1 else 1)

    def o_block(l, src, half):
        size = ob.shape[2] // len(halves(l))
        return ob.at[l, src, pl.ds(half * size, size)]

    def o_copy(l, src, half, send, to_sp):
        at = src // 2 if l == 0 else n // 2 + src // 2 * 2 + half
        return same(o_block(l, src, half), send, osem.at[at], to_sp)

    def o_core(l, src, half):
        at = src // 4 if l == 0 else levels + src // 2
        same(o_block(l, src, half), coresem, ocsem.at[at], twin).start()

    def o_swap(l):
        return remote(osw.at[l], ob.at[l, twin], swsem.at[0], swsem.at[1 + l], twin, peer)

    def o_take(l, src, half):
        o_copy(l, src, half, sidesem, side).wait_recv()

    def o_up(l, src, half):
        pl.when(has_up)(lambda: o_copy(l, src, half, upsem, sp + 4).start())

    def o_down(l, src, half):
        pl.when(has_down)(lambda: o_copy(l, src, half, downsem, sp - 4).start())

    def o_here(l, src, half):
        o_copy(l, src, half, sidesem, side).start()
        o_core(l, src, half)

    def o_swapped(l):
        pl.when(swaps)(lambda: o_swap(l).wait_recv())

    def o_own_line(l, up, down):
        for half in halves(l):
            pl.when(up)(lambda: o_up(l, sp, half))
            pl.when(down)(lambda: o_down(l, sp, half))

    def o_own_here(l):
        for half in halves(l):
            o_here(l, sp, half)

    def o_line(l, d, below=True, above=True):
        def one(zz, onward):
            src = index(zz, y, core)
            for half in halves(l):
                o_take(l, src, half)
                onward(l, src, half)
                if l == LAYERS - 1 and d == 1:
                    pl.when(middle)(lambda: o_copy(l, src, half, sidesem, side).start())
                    o_core(l, src, half)
                else:
                    o_here(l, src, half)

        pl.when(jnp.logical_and(z - d >= 0, below))(lambda: one(z - d, o_up))
        pl.when(jnp.logical_and(z + d < levels, above))(lambda: one(z + d, o_down))

    def o_across(l, zz):
        src = index(zz, 1 - y, core)
        for half in halves(l):
            o_take(l, src, half)
            o_core(l, src, half)

    def o_across_end(l):
        src = index(z, 1 - y, core)
        for half in halves(l):
            pl.when(z == 1)(lambda: o_copy(l, src, half, downsem, sp - 4).start())
            pl.when(z == levels - 2)(lambda: o_copy(l, src, half, upsem, sp + 4).start())

    def o_other_both(zz):
        landed(ob.at[0, 0:2], ocsem.at[zz])

    def o_other(zz, yy):
        landed(ob.at[0, 0], ocsem.at[levels + zz * 2 + yy])

    lo = lax.broadcasted_iota(jnp.int32, (depth, LAYERS * depth), 0)
    hi = lax.broadcasted_iota(jnp.int32, (depth, LAYERS * depth), 1)
    clo = lax.broadcasted_iota(jnp.int32, (LAYERS * width, width), 1)
    chi = lax.broadcasted_iota(jnp.int32, (LAYERS * width, width), 0)

    def pick_rows(l):
        pick = (hi == LAYERS * lo + l).astype(jnp.float32).astype(jnp.bfloat16)
        for yy, keep in ((1 - y, False), (y, True)):
            here = pl.ds(pl.multiple_of(yy * quarter, 128), quarter)
            for kind, ref in enumerate((v_ref, g_ref)):
                picked = jnp.dot(pick, ref[:, here], preferred_element_type=jnp.float32).astype(jnp.bfloat16)
                at = kind * quarter
                if keep:
                    vg[l * n + sp, :, at : at + quarter] = picked
                else:
                    gv[l, :, at : at + quarter] = picked

    def pick_columns(l):
        pick = (chi == LAYERS * clo + l).astype(jnp.float32).astype(jnp.bfloat16)
        picked = jnp.dot(o_ref[...], pick, preferred_element_type=jnp.float32).astype(jnp.bfloat16)

        @pl.when(swaps)
        def _():
            osw[l] = picked
            o_swap(l).start()

        @pl.when(jnp.logical_not(swaps))
        def _():
            ob[l, sp] = picked

    def x_side():
        return same(xs.at[y, tp], sidesem, xrsem.at[0], side)

    def x_peer(far):
        block = xs.at[1 - y if far else y, tp]
        return remote(block, block, xsem, xrsem.at[1 + far], sp, peer)

    def square_sum(value):
        return jnp.sum(value * value, axis=1, keepdims=True)

    def normalise_first(yy):
        total = jnp.zeros((rows, 1), jnp.float32)
        for half in range(2):
            total = total + square_sum(xs[yy, half].astype(jnp.float32))
        scale = lax.rsqrt(total / D + EPS)
        for half in range(2):
            gain = ng_ref[0:1, half * cols : (half + 1) * cols]
            nb[yy, :, half * cols : (half + 1) * cols] = (
                xs[yy, half].astype(jnp.float32) * scale * gain).astype(jnp.bfloat16)

    def normalise_next(yy):
        total = jnp.zeros((rows, 1), jnp.float32)
        for half in range(2):
            for zz in range(levels):
                for part in range(2):
                    total = total + square_sum(x1[yy, half, zz, part].astype(jnp.float32))
        scale = lax.rsqrt(total / D + EPS)
        for half in range(2):
            for zz in range(levels):
                for part in range(2):
                    at = index(zz, part, half) * width
                    value = x1[yy, half, zz, part].astype(jnp.float32)
                    nb[yy, :, at : at + width] = (
                        value * scale * ng_ref[1:2, at : at + width]).astype(jnp.bfloat16)

    def gl_copy(l, half):
        here = pl.ds(half * (rows // 2), rows // 2)
        return remote(gs.at[l, here], gr.at[l, here], sidesem, glsem.at[l], side, tp)

    def halo(l, yy):
        return remote(
            gl.at[l, yy], ext.at[l, y, pl.ds(0, HALO)],
            hssem.at[yy], hsem.at[l, y], index(z, yy, core) + 1, tp)

    def halo_wait(l, q):
        remote(
            gl.at[l, 0], ext.at[l, q, pl.ds(0, HALO)],
            hssem.at[0], hsem.at[l, q], side, tp).wait_recv()

    def glu(l):
        weights = vg[l * n : (l + 1) * n].reshape(n * depth, 2 * quarter)

        def tokens(yy):
            both = jnp.dot(nb[yy], weights, preferred_element_type=jnp.float32)
            return both[:, :quarter] * jax.nn.sigmoid(both[:, quarter:])

        theirs = tokens(1 - y)
        gs[l] = theirs.astype(jnp.bfloat16)
        gl[l, 1 - y] = theirs[rows - HALO :]
        for half in (1, 0):
            gl_copy(l, half).start()
        pl.when(follows(1 - y))(lambda: halo(l, 1 - y).start())
        mine = tokens(y)
        ext[l, y, HALO:] = mine
        gl[l, y] = mine[rows - HALO :]
        pl.when(follows(y))(lambda: halo(l, y).start())

    def cv_copy(l, q, half):
        here = pl.ds(half * (rows // 2), rows // 2)
        return remote(cvs.at[l, q, here], cvr.at[l, q, here], xsem, cvsem.at[l], sp, peer)

    def conv_rows(l, q, r0):
        tap_cols = pl.ds(pl.multiple_of((tp * 2 + q) * quarter, 128), quarter)
        running = jnp.zeros((HALO, quarter), jnp.float32)
        for k in range(KW):
            at = r0 + k + HALO - (KW - 1)
            running = running + taps_ref[k, l : l + 1, tap_cols] * ext[l, q, at : at + HALO]
        cv[q, r0 : r0 + HALO] = running
        cvs[l, q, r0 : r0 + HALO] = running.astype(jnp.bfloat16)

    def conv(l, q):
        for half in (1, 0):
            for r0 in range(half * rows // 2 + (HALO if half == 0 else 0), (half + 1) * rows // 2, HALO):
                conv_rows(l, q, r0)
            if half == 0:
                pl.when(sp > 0)(lambda: halo_wait(l, q))
                conv_rows(l, q, 0)
            cv_copy(l, q, half).start()

    def take_glu(l):
        landed(gr.at[l], glsem.at[l])
        ext[l, 1 - y, HALO:] = gr[l].astype(jnp.float32)

    def activate(l, between):
        first = jnp.zeros((rows, 1), jnp.float32)
        second = jnp.zeros((rows, 1), jnp.float32)
        for q in range(2):
            value = cv[q]
            first = first + jnp.sum(value, axis=1, keepdims=True)
            second = second + square_sum(value)
        landed(cvr.at[l], cvsem.at[l])
        between()
        for q in range(2):
            value = cvr[l, q].astype(jnp.float32)
            first = first + jnp.sum(value, axis=1, keepdims=True)
            second = second + square_sum(value)
        mean = first / C
        scale = lax.rsqrt(second / C - mean * mean + EPS)
        for half, source in ((tp, None), (peer, cvr)):
            for q in range(2):
                value = cv[q] if source is None else source[l, q].astype(jnp.float32)
                here = pl.ds(pl.multiple_of((half * 2 + q) * quarter, 128), quarter)
                v = (value - mean) * scale * lng_ref[l : l + 1, here] + lnb_ref[l : l + 1, here]
                act[half, :, q * quarter : (q + 1) * quarter] = (v / (1.0 + jnp.exp(-v))).astype(jnp.bfloat16)

    def branch(l, zz):
        total = None
        for cc in range(2):
            weights = jnp.concatenate([ob[l, index(zz, 0, cc)], ob[l, index(zz, 1, cc)]], axis=1)
            partial_sum = jnp.dot(act[cc], weights, preferred_element_type=jnp.float32)
            partial_sum = partial_sum.astype(jnp.bfloat16).astype(jnp.float32)
            total = partial_sum if total is None else total + partial_sum
        return total

    def x1_side(zz):
        return same(x1.at[y, tp, zz], sidesem, x1sem.at[0, zz], side)

    def x1_peer(far, zz):
        block = x1.at[1 - y if far else y, tp, zz]
        return remote(block, block, xsem, x1sem.at[1 + far, zz], sp, peer)

    def x1_diagonal(zz):
        return same(x1.at[y, peer, zz], sidesem, x1sem.at[2, zz], side)

    def step(i):
        return (z + levels + (1 - 2 * (z // half_levels)) * i) % levels

    def project_first(zz):
        o_other_both(zz)
        added = branch(0, zz)
        for part in range(2):
            at = pl.ds(pl.multiple_of((index(zz, part, tp) % (n // 2)) * width, 128), width)
            here = xs[y, zz // half_levels, :, at].astype(jnp.float32)
            x1[y, tp, zz, part] = (
                here + added[:, part * width : (part + 1) * width]).astype(jnp.bfloat16)
        x1_side(zz).start()
        x1_peer(0, zz).start()

    def x2_copy(zz, part):
        return remote(x2.at[zz, part], x2r.at[zz, part], xsem, x2sem, sp, peer)

    def put_last(zz, part, added):
        fresh = (x1[y, tp, zz, part].astype(jnp.float32) + added).astype(jnp.bfloat16)
        x2[zz, part] = fresh
        pl.when(zz // half_levels == peer)(lambda: x2_copy(zz, part).start())
        return square_sum(fresh.astype(jnp.float32))

    def project_last(zz):
        o_other(zz, y)
        o_other(zz, 1 - y)
        added = branch(1, zz)
        return put_last(zz, 0, added[:, :width]) + put_last(zz, 1, added[:, width:])

    def project_part(zz, part):
        o_other(zz, part)
        added = None
        for cc in range(2):
            one = jnp.dot(act[cc], ob[1, index(zz, part, cc)], preferred_element_type=jnp.float32)
            one = one.astype(jnp.bfloat16).astype(jnp.float32)
            added = one if added is None else added + one
        return put_last(zz, part, added)

    def stat_copy():
        return remote(st, rst, tsem.at[0], tsem.at[1], sp, peer)

    landed(vg.at[0 : 2 * LAYERS], isem.at[0])
    pick_rows(0)

    @pl.when(sp == 0)
    def _():
        for l in range(LAYERS):
            for q in range(2):
                ext[l, q, 0:HALO] = jnp.zeros((HALO, quarter), jnp.float32)

    ends = [has_up, has_down, swaps, follows(0), follows(1)]
    pl.semaphore_wait(barrier, 3 + sum(end.astype(jnp.int32) for end in ends))

    for half in range(gives(0)):
        vg_give(0, half).start()
    vg_own(0)
    loads[2].wait()
    x_peer(0).start()
    x_side().start()
    pick_rows(1)
    for half in range(gives(1)):
        vg_give(1, half).start()
    loads[3].wait()
    for l in range(LAYERS):
        pick_columns(l)
    for load in loads[4:]:
        load.wait()
    vg_side(0)
    for d in near:
        vg_line(0, d)
        if d == 1:
            x_peer(0).wait_recv()
            normalise_first(y)
            o_swapped(0)
            pl.when(last)(lambda: o_own_line(0, has_up, has_down))
            x_side().wait_recv()
            x_peer(1).start()
    pl.when(middle)(lambda: o_own_line(0, lower, upper))
    o_own_here(0)
    vg_line(0, levels - 1)
    x_peer(1).wait_recv()
    normalise_first(1 - y)
    vg_other(0)
    pl.when(middle)(lambda: o_own_line(0, upper, lower))
    glu(0)

    def o_near(l, *distances):
        for d in distances:
            o_line(l, d)

    pl.when(middle)(lambda: o_near(0, *near))
    vg_own(1)
    vg_side(1)
    o_swapped(1)
    pl.when(last)(lambda: o_own_line(1, has_up, has_down))
    conv(0, y)
    pl.when(last)(lambda: o_near(0, 1))
    take_glu(0)
    conv(0, 1 - y)
    o_across(0, step(0))
    pl.when(last)(lambda: o_near(0, *near[1:], levels - 1))
    activate(0, lambda: o_across(0, step(1)))
    project_first(step(0))
    o_across(0, step(2))
    project_first(step(1))
    pl.when(middle)(lambda: vg_line(1, 1))
    for i in range(2, levels):
        if i > 2:
            o_across(0, step(i))
        project_first(step(i))
    pl.when(last)(lambda: vg_line(1, 1))
    for i in range(0, levels, 2):
        x1_peer(0, step(i)).wait_recv()
        x1_peer(0, step(i + 1)).wait_recv()
        x1_diagonal(step(i + 1)).start()
        x1_side(step(i)).wait_recv()
        x1_peer(1, step(i)).start()
        x1_side(step(i + 1)).wait_recv()
    for d in near[1:]:
        vg_line(1, d)
    normalise_next(y)
    pl.when(middle)(lambda: o_own_line(1, lower, upper))
    o_own_here(1)

    @pl.when(middle)
    def _():
        for d in near:
            o_line(1, d, lower, upper)

    for i in range(levels):
        if i % 2 == 0:
            x1_peer(1, step(i)).wait_recv()
        else:
            x1_diagonal(step(i)).wait_recv()
    normalise_next(1 - y)
    vg_line(1, levels - 1)
    early = jnp.logical_and(last, core == 1)
    late = jnp.logical_and(last, core == 0)
    pl.when(early)(lambda: o_near(1, 2))
    vg_other(1)
    glu(1)

    @pl.when(middle)
    def _():
        for d in near:
            o_line(1, d, upper, lower)
        o_own_line(1, upper, lower)
        o_across(1, z)
        o_across_end(1)

    conv(1, y)
    pl.when(early)(lambda: o_near(1, *range(3, levels)))
    pl.when(late)(lambda: o_near(1, 2))
    take_glu(1)
    conv(1, 1 - y)
    pl.when(last)(lambda: o_across(1, z))
    pl.when(early)(lambda: o_near(1, 1))
    pl.when(late)(lambda: o_near(1, *range(3, levels), 1))
    at_end = last.astype(jnp.int32)

    def order(i):
        if i == 0:
            return step(0)
        return step(i + at_end if i < levels - 1 else levels - 1 - at_end * (levels - 2))

    activate(1, lambda: None)
    squares = project_last(order(0))

    @pl.when(core == 1)
    def _():
        for i in range(1, levels):
            o_across(1, order(i))

    squares = squares + project_part(order(levels - 1), y)
    for i in near:
        pl.when(core == 0)(lambda: o_across(1, order(i)))
        squares = squares + project_last(order(i))
    pl.when(core == 0)(lambda: o_across(1, order(levels - 1)))
    squares = squares + project_part(order(levels - 1), 1 - y)
    st[...] = jnp.broadcast_to(squares, (rows, 128)).T[0:8]
    stat_copy().start()

    for zz in range(levels):
        @pl.when(z == zz)
        def _():
            for sem, count in ((upsem, zz + 1 if zz < levels - 1 else 0), (downsem, levels - zz if zz > 0 else 0)):
                count *= 3 * LAYERS
                extra = (zz == levels - 2) if sem is upsem else (zz == 1)
                if count:
                    landed(vg.at[0 : count + extra], sem)
    landed(vg.at[0 : 2 * n], coresem)
    count = LAYERS + LAYERS * levels + 2 + levels // 2 + levels // 4 + LAYERS // 2
    pl.when(middle)(lambda: landed(vg.at[0:count], sidesem))
    pl.when(last)(lambda: landed(vg.at[0 : count - 1], sidesem))
    pl.when(swaps)(lambda: landed(osw, swsem.at[0]))
    for yy in range(2):
        pl.when(follows(yy))(lambda: landed(gl.at[0], hssem.at[yy]))

    stat_copy().wait_recv()
    landed(x2r.at[0:half_levels], x2sem)
    both = st[...] + rst[...]
    total = jnp.concatenate([both] * (128 // 8), axis=0).T[:, 0:1]
    scale = lax.rsqrt(total / D + EPS)
    for i in range(half_levels):
        zz = tp * half_levels + i
        for part in range(2):
            for source, parity in ((x2, tp), (x2r, peer)):
                at = ((i * 2 + part) * 2 + parity) * width
                gain = fg_ref[0:1, pl.ds(pl.multiple_of(tp * cols + at, 128), width)]
                value = source[zz, part].astype(jnp.float32)
                out_ref[:, pl.ds(pl.multiple_of(at, 128), width)] = (value * scale * gain).astype(jnp.bfloat16)
    landed(vg.at[0 : 4 + levels // 2 + levels // 4 + LAYERS + levels // 4], xsem)
    stat_copy().wait_send()


def fused(n, stream, norm_gain, value_weight, gate_weight, conv_taps, ln_gain, ln_bias, out_weight, final_gain):
    rows, cols = stream.shape
    depth, ch = value_weight.shape[0] // LAYERS, value_weight.shape[1]
    width = out_weight.shape[1] // LAYERS
    levels = n // 4
    bf16, f32 = jnp.bfloat16, jnp.float32
    dma = pltpu.SemaphoreType.DMA
    arrays = (stream, norm_gain, value_weight, gate_weight, conv_taps.transpose(1, 0, 2),
              ln_gain, ln_bias, out_weight, final_gain.reshape(1, -1))
    return pl.pallas_call(
        functools.partial(fused_kernel, n),
        out_shape=pltpu.VMEM((rows, cols), bf16),
        in_specs=[pl.BlockSpec(memory_space=pl.ANY)] * 9,
        out_specs=pl.BlockSpec(memory_space=pltpu.VMEM),
        scratch_shapes=[pltpu.VMEM(array.shape, array.dtype) for array in arrays[1:]] + [
            dma((len(arrays) - 1,)),
            pltpu.VMEM((LAYERS * n, depth, ch), bf16),
            pltpu.VMEM((LAYERS, depth, ch), bf16),
            pltpu.VMEM((LAYERS, n, ch, width), bf16),
            pltpu.VMEM((LAYERS, ch, width), bf16),
            pltpu.VMEM((2, 2, rows, cols), bf16),
            pltpu.VMEM((2, 2, levels, 2, rows, width), bf16),
            pltpu.VMEM((levels, 2, rows, width), bf16),
            pltpu.VMEM((levels, 2, rows, width), bf16),
            pltpu.VMEM((2, rows, 2 * cols), bf16),
            pltpu.VMEM((LAYERS, 2, HALO, ch // 2), f32),
            pltpu.VMEM((LAYERS, rows, ch // 2), bf16),
            pltpu.VMEM((LAYERS, rows, ch // 2), bf16),
            pltpu.VMEM((LAYERS, 2, HALO + rows, ch // 2), f32),
            pltpu.VMEM((2, rows, ch // 2), f32),
            pltpu.VMEM((LAYERS, 2, rows, ch // 2), bf16),
            pltpu.VMEM((LAYERS, 2, rows, ch // 2), bf16),
            pltpu.VMEM((2, rows, ch), bf16),
            pltpu.VMEM((8, rows), f32),
            pltpu.VMEM((8, rows), f32),
            dma, dma, dma, dma, dma,
            dma((LAYERS + 1,)),
            dma((LAYERS, n // 2)),
            dma((LAYERS,)),
            dma((n // 2 + n,)),
            dma((levels + n // 2,)),
            dma((1 + LAYERS,)),
            dma((3,)),
            dma((3, levels)),
            dma,
            dma((LAYERS,)),
            dma((LAYERS,)),
            dma((2,)),
            dma((LAYERS, 2)),
            dma((2,)),
        ],
        compiler_params=pltpu.CompilerParams(collective_id=0, has_side_effects=True),
    )(*arrays)


def solution(mesh):
    placed = (P("sp", "tp"), P(), P("sp", "tp"), P("sp", "tp"), P(), P(), P(), P("tp", "sp"), P())
    n, n_tp = mesh.shape["sp"], mesh.shape["tp"]

    def step(*args):
        stream, out_weight = args[0], args[7]
        fits = (n_tp == 2 and n % 8 == 0 and n > 8 and stream.shape[0] == 128 and out_weight.shape[1] == 128 * LAYERS
                and args[2].shape == (128 * LAYERS, 512))
        return fused(n, *args) if fits else local(*args)

    return jax.shard_map(step, mesh=mesh, in_specs=placed, out_specs=P("sp", "tp"), check_vma=False)
```

```python
import functools

import jax
import jax.numpy as jnp
from jax import lax
from jax.experimental import pallas as pl
from jax.experimental.pallas import tpu as pltpu
from jax.sharding import PartitionSpec as P

D = 2048
C = 1024
KW = 31
LAYERS = 2


EPS = 1e-06


def from_behind(value, axis, steps):
    count = lax.axis_size(axis)
    first, last = (max(0, -steps), min(count, count - steps))
    return lax.ppermute(value, axis, [(source, source + steps) for source in range(first, last)])


def valid_conv(extended, tap_table):
    length = extended.shape[0] - (KW - 1)
    running = tap_table[0] * extended[0:length]
    for tap_index in range(1, KW):
        running = running + tap_table[tap_index] * extended[tap_index : tap_index + length]
    return running


def local(
    stream,
    norm_gain,
    value_weight,
    gate_weight,
    conv_taps,
    ln_gain,
    ln_bias,
    out_weight,
    final_gain,
):
    tokens_here = stream.shape[0]
    columns = stream.shape[1]
    channels = value_weight.shape[1]
    rim_rows = KW - 1
    tp_index = lax.axis_index("tp")
    my_taps = lax.dynamic_slice_in_dim(conv_taps, tp_index * channels, channels, 2)
    my_ln_gain = lax.dynamic_slice_in_dim(ln_gain, tp_index * channels, channels, 1)
    my_ln_bias = lax.dynamic_slice_in_dim(ln_bias, tp_index * channels, channels, 1)
    my_final = lax.dynamic_slice_in_dim(final_gain, tp_index * columns, columns, 0)
    value_all, gate_all, out_all = (
        lax.all_gather(value_weight, "sp", axis=0, tiled=True),
        lax.all_gather(gate_weight, "sp", axis=0, tiled=True),
        lax.all_gather(out_weight, "sp", axis=1, tiled=True),
    )
    value_all = value_all.reshape(D, LAYERS, channels)
    gate_all = gate_all.reshape(D, LAYERS, channels)
    out_all = out_all.reshape(channels, D, LAYERS)
    earlier = from_behind(stream[-LAYERS * rim_rows :], "sp", 1)
    current = jnp.concatenate([earlier, stream], axis=0)
    for layer_index in range(LAYERS):
        prefix = (LAYERS - layer_index) * rim_rows
        gathered = lax.all_gather(current, "tp", axis=1, tiled=True)
        gathered32 = gathered.astype(jnp.float32)
        scale = lax.rsqrt(jnp.sum(gathered32 * gathered32, axis=1, keepdims=True) / D + EPS)
        run_normed = (gathered32 * scale * norm_gain[layer_index]).astype(jnp.bfloat16)
        value_proj = jnp.dot(
            run_normed, value_all[:, layer_index], preferred_element_type=jnp.float32
        )
        gate_proj = jnp.dot(
            run_normed, gate_all[:, layer_index], preferred_element_type=jnp.float32
        )
        glu_out = value_proj * jax.nn.sigmoid(gate_proj)
        positions = (
            lax.axis_index("sp") * tokens_here - prefix + lax.iota(jnp.int32, current.shape[0])
        )
        extended = jnp.where((positions >= 0)[:, None], glu_out, 0.0)
        residual = current[rim_rows:].astype(jnp.float32)
        conv_out = valid_conv(extended, my_taps[layer_index])
        first_sums, square_sums = lax.psum(
            (jnp.sum(conv_out, axis=1), jnp.sum(conv_out * conv_out, axis=1)), "tp"
        )
        row_mean = (first_sums / C)[:, None]
        row_var = (square_sums / C)[:, None] - row_mean * row_mean
        run_active = jax.nn.silu(
            (conv_out - row_mean) * lax.rsqrt(row_var + EPS) * my_ln_gain[layer_index]
            + my_ln_bias[layer_index]
        ).astype(jnp.bfloat16)
        partial_value = jnp.dot(
            run_active, out_all[:, :, layer_index], preferred_element_type=jnp.float32
        )
        summed = lax.psum_scatter(
            partial_value.astype(jnp.bfloat16), "tp", scatter_dimension=1, tiled=True
        ).astype(jnp.float32)
        current = (residual + summed).astype(jnp.bfloat16)
    final32 = current.astype(jnp.float32)
    squares = lax.psum(jnp.sum(final32 * final32, axis=1), "tp")
    return (final32 * lax.rsqrt(squares[:, None] / D + EPS) * my_final).astype(jnp.bfloat16)


MESH = pl.DeviceIdType.MESH
HALO = 32


def fused_kernel(
    n, x_in, ng_in, v_in, g_in, taps_in, lng_in, lnb_in, o_in, fg_in, out_ref,
    ng_ref, v_ref, g_ref, taps_ref, lng_ref, lnb_ref, o_ref, fg_ref, isem,
    vg, gv, ob, osw, xs, x1, x2, x2r, nb, gl, gs, gr, ext, cv, cvs, cvr, act, st, rst,
    upsem, downsem, sidesem, coresem, xsem, gvsem, vgsem, vcsem, osem, ocsem, swsem, xrsem, x1sem, x2sem, cvsem, glsem, hssem, hsem, tsem,
):
    levels = n // 4
    half_levels = levels // 2
    sp = lax.axis_index("sp")
    tp = lax.axis_index("tp")
    z, y, core = sp // 4, (sp // 2) % 2, sp % 2
    peer = 1 - tp
    rows, cols = xs.shape[2], xs.shape[3]
    depth, quarter = vg.shape[1], vg.shape[2] // 2
    width = ob.shape[3]
    has_up, has_down = z < levels - 1, z > 0
    swaps = tp + core == 1
    middle = jnp.logical_and(has_up, has_down)
    last = jnp.logical_not(middle)
    near = range(1, levels - 1)
    lower, upper = z < half_levels, z >= half_levels
    side, twin = sp + 2 - 4 * y, sp + 1 - 2 * core

    def index(zz, yy, cc):
        return (zz * 2 + yy) * 2 + cc

    def landed(block, sem):
        pltpu.make_async_copy(block, block, sem).wait()

    def remote(src, dst, send, recv, to_sp, to_tp):
        return pltpu.make_async_remote_copy(
            src_ref=src, dst_ref=dst, send_sem=send, recv_sem=recv,
            device_id={"sp": to_sp, "tp": to_tp}, device_id_type=MESH)

    def same(ref, send, recv, to_sp):
        return remote(ref, ref, send, recv, to_sp, tp)

    barrier = pltpu.get_barrier_semaphore()

    def greet(to_sp, to_tp):
        pl.semaphore_signal(barrier, inc=1, device_id={"sp": to_sp, "tp": to_tp}, device_id_type=MESH)

    greet(side, tp)
    greet(twin, tp)
    greet(sp, peer)
    pl.when(has_up)(lambda: greet(sp + 4, tp))
    pl.when(has_down)(lambda: greet(sp - 4, tp))
    pl.when(swaps)(lambda: greet(twin, peer))
    before = sp - 1

    @pl.when(sp > 0)
    def _():
        for yy in range(2):
            greet(index(before // 4, yy, before % 2), tp)

    loads = [
        pltpu.make_async_copy(source, to, isem.at[max(i - 1, 0)])
        for i, (source, to) in enumerate((
            (v_in, v_ref), (g_in, g_ref), (x_in, xs.at[y, tp]), (o_in, o_ref), (ng_in, ng_ref),
            (taps_in, taps_ref), (lng_in, lng_ref), (lnb_in, lnb_ref), (fg_in, fg_ref)))
    ]
    for load in loads:
        load.start()

    def follows(yy):
        return index(z, yy, core) + 1 < n

    def vg_copy(l, src, send, to_sp):
        return same(vg.at[l * n + src], send, vgsem.at[l, src // 2], to_sp)

    def gives(l):
        return 2 if l == 0 else 1

    def vg_rows(l, half):
        return pl.ds(half * (depth // gives(l)), depth // gives(l))

    def vg_give(l, half):
        here = vg_rows(l, half)
        return remote(
            gv.at[l, here], vg.at[l * n + sp, here], sidesem, gvsem.at[half if l == 0 else l + 1], side, tp)

    def vg_take(l, src):
        vg_copy(l, src, coresem, twin).wait_recv()

    def vg_up(l, src):
        pl.when(has_up)(lambda: vg_copy(l, src, upsem, sp + 4).start())

    def vg_down(l, src):
        pl.when(has_down)(lambda: vg_copy(l, src, downsem, sp - 4).start())

    def vg_core(l, src):
        same(vg.at[l * n + src], coresem, vcsem.at[l], twin).start()

    def vg_own(l):
        vg_up(l, sp)
        vg_down(l, sp)
        vg_core(l, sp)

    def vg_side(l):
        src = index(z, 1 - y, core)
        for half in range(gives(l)):
            vg_give(l, half).wait_recv()
            block = vg.at[l * n + src, vg_rows(l, half)]
            pl.when(has_up)(lambda: same(block, upsem, vgsem.at[l, src // 2], sp + 4).start())
            pl.when(has_down)(lambda: same(block, downsem, vgsem.at[l, src // 2], sp - 4).start())
        vg_core(l, src)

    def vg_line(l, d):
        def one(zz, onward):
            for yy in (y, 1 - y):
                src = index(zz, yy, core)
                vg_take(l, src)
                onward(l, src)
                vg_core(l, src)

        pl.when(z - d >= 0)(lambda: one(z - d, vg_up))
        pl.when(z + d < levels)(lambda: one(z + d, vg_down))

    def vg_other(l):
        landed(vg.at[0 : n // 2], vcsem.at[l])

    def halves(l):
        return range(2 if l == LAYERS - 1 else 1)

    def o_block(l, src, half):
        size = ob.shape[2] // len(halves(l))
        return ob.at[l, src, pl.ds(half * size, size)]

    def o_copy(l, src, half, send, to_sp):
        at = src // 2 if l == 0 else n // 2 + src // 2 * 2 + half
        return same(o_block(l, src, half), send, osem.at[at], to_sp)

    def o_core(l, src, half):
        at = src // 4 if l == 0 else levels + src // 2
        same(o_block(l, src, half), coresem, ocsem.at[at], twin).start()

    def o_swap(l):
        return remote(osw.at[l], ob.at[l, twin], swsem.at[0], swsem.at[1 + l], twin, peer)

    def o_take(l, src, half):
        o_copy(l, src, half, sidesem, side).wait_recv()

    def o_up(l, src, half):
        pl.when(has_up)(lambda: o_copy(l, src, half, upsem, sp + 4).start())

    def o_down(l, src, half):
        pl.when(has_down)(lambda: o_copy(l, src, half, downsem, sp - 4).start())

    def o_here(l, src, half):
        o_copy(l, src, half, sidesem, side).start()
        o_core(l, src, half)

    def o_swapped(l):
        pl.when(swaps)(lambda: o_swap(l).wait_recv())

    def o_own_line(l, up, down):
        for half in halves(l):
            pl.when(up)(lambda: o_up(l, sp, half))
            pl.when(down)(lambda: o_down(l, sp, half))

    def o_own_here(l):
        for half in halves(l):
            o_here(l, sp, half)

    def o_line(l, d, below=True, above=True):
        def one(zz, onward):
            src = index(zz, y, core)
            for half in halves(l):
                o_take(l, src, half)
                onward(l, src, half)
                if l == LAYERS - 1 and d == 1:
                    pl.when(middle)(lambda: o_copy(l, src, half, sidesem, side).start())
                    o_core(l, src, half)
                else:
                    o_here(l, src, half)

        pl.when(jnp.logical_and(z - d >= 0, below))(lambda: one(z - d, o_up))
        pl.when(jnp.logical_and(z + d < levels, above))(lambda: one(z + d, o_down))

    def o_across(l, zz):
        src = index(zz, 1 - y, core)
        for half in halves(l):
            o_take(l, src, half)
            o_core(l, src, half)

    def o_across_end(l):
        src = index(z, 1 - y, core)
        for half in halves(l):
            pl.when(z == 1)(lambda: o_copy(l, src, half, downsem, sp - 4).start())
            pl.when(z == levels - 2)(lambda: o_copy(l, src, half, upsem, sp + 4).start())

    def o_other_both(zz):
        landed(ob.at[0, 0:2], ocsem.at[zz])

    def o_other(zz, yy):
        landed(ob.at[0, 0], ocsem.at[levels + zz * 2 + yy])

    lo = lax.broadcasted_iota(jnp.int32, (depth, LAYERS * depth), 0)
    hi = lax.broadcasted_iota(jnp.int32, (depth, LAYERS * depth), 1)
    clo = lax.broadcasted_iota(jnp.int32, (LAYERS * width, width), 1)
    chi = lax.broadcasted_iota(jnp.int32, (LAYERS * width, width), 0)

    def pick_rows(l):
        pick = (hi == LAYERS * lo + l).astype(jnp.float32).astype(jnp.bfloat16)
        for yy, keep in ((1 - y, False), (y, True)):
            here = pl.ds(pl.multiple_of(yy * quarter, 128), quarter)
            for kind, ref in enumerate((v_ref, g_ref)):
                picked = jnp.dot(pick, ref[:, here], preferred_element_type=jnp.float32).astype(jnp.bfloat16)
                at = kind * quarter
                if keep:
                    vg[l * n + sp, :, at : at + quarter] = picked
                else:
                    gv[l, :, at : at + quarter] = picked

    def pick_columns(l):
        pick = (chi == LAYERS * clo + l).astype(jnp.float32).astype(jnp.bfloat16)
        picked = jnp.dot(o_ref[...], pick, preferred_element_type=jnp.float32).astype(jnp.bfloat16)

        @pl.when(swaps)
        def _():
            osw[l] = picked
            o_swap(l).start()

        @pl.when(jnp.logical_not(swaps))
        def _():
            ob[l, sp] = picked

    def x_side():
        return same(xs.at[y, tp], sidesem, xrsem.at[0], side)

    def x_peer(far):
        block = xs.at[1 - y if far else y, tp]
        return remote(block, block, xsem, xrsem.at[1 + far], sp, peer)

    def square_sum(value):
        return jnp.sum(value * value, axis=1, keepdims=True)

    def normalise_first(yy):
        total = jnp.zeros((rows, 1), jnp.float32)
        for half in range(2):
            total = total + square_sum(xs[yy, half].astype(jnp.float32))
        scale = lax.rsqrt(total / D + EPS)
        for half in range(2):
            gain = ng_ref[0:1, half * cols : (half + 1) * cols]
            nb[yy, :, half * cols : (half + 1) * cols] = (
                xs[yy, half].astype(jnp.float32) * scale * gain).astype(jnp.bfloat16)

    def normalise_next(yy):
        total = jnp.zeros((rows, 1), jnp.float32)
        for half in range(2):
            for zz in range(levels):
                for part in range(2):
                    total = total + square_sum(x1[yy, half, zz, part].astype(jnp.float32))
        scale = lax.rsqrt(total / D + EPS)
        for half in range(2):
            for zz in range(levels):
                for part in range(2):
                    at = index(zz, part, half) * width
                    value = x1[yy, half, zz, part].astype(jnp.float32)
                    nb[yy, :, at : at + width] = (
                        value * scale * ng_ref[1:2, at : at + width]).astype(jnp.bfloat16)

    def gl_copy(l, half):
        here = pl.ds(half * (rows // 2), rows // 2)
        return remote(gs.at[l, here], gr.at[l, here], sidesem, glsem.at[l], side, tp)

    def halo(l, yy):
        return remote(
            gl.at[l, yy], ext.at[l, y, pl.ds(0, HALO)],
            hssem, hsem.at[l, y], index(z, yy, core) + 1, tp)

    def halo_wait(l, q):
        remote(
            gl.at[l, 0], ext.at[l, q, pl.ds(0, HALO)],
            hssem, hsem.at[l, q], side, tp).wait_recv()

    def glu(l):
        weights = vg[l * n : (l + 1) * n].reshape(n * depth, 2 * quarter)

        def tokens(yy):
            both = jnp.dot(nb[yy], weights, preferred_element_type=jnp.float32)
            return both[:, :quarter] * jax.nn.sigmoid(both[:, quarter:])

        theirs = tokens(1 - y)
        gs[l] = theirs.astype(jnp.bfloat16)
        gl[l, 1 - y] = theirs[rows - HALO :]
        for half in (1, 0):
            gl_copy(l, half).start()
        pl.when(follows(1 - y))(lambda: halo(l, 1 - y).start())
        mine = tokens(y)
        ext[l, y, HALO:] = mine
        gl[l, y] = mine[rows - HALO :]
        pl.when(follows(y))(lambda: halo(l, y).start())

    def cv_copy(l, q, half):
        here = pl.ds(half * (rows // 2), rows // 2)
        return remote(cvs.at[l, q, here], cvr.at[l, q, here], xsem, cvsem.at[l], sp, peer)

    def conv_rows(l, q, r0):
        tap_cols = pl.ds(pl.multiple_of((tp * 2 + q) * quarter, 128), quarter)
        running = jnp.zeros((HALO, quarter), jnp.float32)
        for k in range(KW):
            at = r0 + k + HALO - (KW - 1)
            running = running + taps_ref[k, l : l + 1, tap_cols] * ext[l, q, at : at + HALO]
        cv[q, r0 : r0 + HALO] = running
        cvs[l, q, r0 : r0 + HALO] = running.astype(jnp.bfloat16)

    def conv(l, q):
        for half in (1, 0):
            for r0 in range(half * rows // 2 + (HALO if half == 0 else 0), (half + 1) * rows // 2, HALO):
                conv_rows(l, q, r0)
            if half == 0:
                pl.when(sp > 0)(lambda: halo_wait(l, q))
                conv_rows(l, q, 0)
            cv_copy(l, q, half).start()

    def take_glu(l):
        landed(gr.at[l], glsem.at[l])
        ext[l, 1 - y, HALO:] = gr[l].astype(jnp.float32)

    def activate(l, between):
        first = jnp.zeros((rows, 1), jnp.float32)
        second = jnp.zeros((rows, 1), jnp.float32)
        for q in range(2):
            value = cv[q]
            first = first + jnp.sum(value, axis=1, keepdims=True)
            second = second + square_sum(value)
        landed(cvr.at[l], cvsem.at[l])
        between()
        for q in range(2):
            value = cvr[l, q].astype(jnp.float32)
            first = first + jnp.sum(value, axis=1, keepdims=True)
            second = second + square_sum(value)
        mean = first / C
        scale = lax.rsqrt(second / C - mean * mean + EPS)
        for half, source in ((tp, None), (peer, cvr)):
            for q in range(2):
                value = cv[q] if source is None else source[l, q].astype(jnp.float32)
                here = pl.ds(pl.multiple_of((half * 2 + q) * quarter, 128), quarter)
                v = (value - mean) * scale * lng_ref[l : l + 1, here] + lnb_ref[l : l + 1, here]
                act[half, :, q * quarter : (q + 1) * quarter] = (v / (1.0 + jnp.exp(-v))).astype(jnp.bfloat16)

    def branch(l, zz):
        total = None
        for cc in range(2):
            weights = jnp.concatenate([ob[l, index(zz, 0, cc)], ob[l, index(zz, 1, cc)]], axis=1)
            partial_sum = jnp.dot(act[cc], weights, preferred_element_type=jnp.float32)
            partial_sum = partial_sum.astype(jnp.bfloat16).astype(jnp.float32)
            total = partial_sum if total is None else total + partial_sum
        return total

    def x1_side(zz):
        return same(x1.at[y, tp, zz], sidesem, x1sem.at[zz], side)

    def x1_peer(far, zz, i):
        block = x1.at[1 - y if far else y, tp, zz]
        return remote(block, block, xsem, x1sem.at[levels + (half_levels if far else i // 2)], sp, peer)

    def x1_diagonal(zz):
        return same(x1.at[y, peer, zz], sidesem, x1sem.at[levels + half_levels + 1], side)

    def step(i):
        return (z + levels + (1 - 2 * (z // half_levels)) * i) % levels

    def project_first(zz, i):
        o_other_both(zz)
        added = branch(0, zz)
        for part in range(2):
            at = pl.ds(pl.multiple_of((index(zz, part, tp) % (n // 2)) * width, 128), width)
            here = xs[y, zz // half_levels, :, at].astype(jnp.float32)
            x1[y, tp, zz, part] = (
                here + added[:, part * width : (part + 1) * width]).astype(jnp.bfloat16)
        x1_side(zz).start()
        x1_peer(0, zz, i).start()

    def x2_copy(zz, part):
        return remote(x2.at[zz, part], x2r.at[zz, part], xsem, x2sem, sp, peer)

    def put_last(zz, part, added):
        fresh = (x1[y, tp, zz, part].astype(jnp.float32) + added).astype(jnp.bfloat16)
        x2[zz, part] = fresh
        pl.when(zz // half_levels == peer)(lambda: x2_copy(zz, part).start())
        return square_sum(fresh.astype(jnp.float32))

    def project_last(zz):
        o_other(zz, y)
        o_other(zz, 1 - y)
        added = branch(1, zz)
        return put_last(zz, 0, added[:, :width]) + put_last(zz, 1, added[:, width:])

    def project_pair(planes, part):
        for zz in planes:
            o_other(zz, part)
        added = None
        for cc in range(2):
            weights = jnp.concatenate([ob[1, index(zz, part, cc)] for zz in planes], axis=1)
            one = jnp.dot(act[cc], weights, preferred_element_type=jnp.float32)
            one = one.astype(jnp.bfloat16).astype(jnp.float32)
            added = one if added is None else added + one
        return sum(put_last(zz, part, added[:, k * width : (k + 1) * width]) for k, zz in enumerate(planes))

    def stat_copy():
        return remote(st, rst, tsem.at[0], tsem.at[1], sp, peer)

    landed(vg.at[0 : 2 * LAYERS], isem.at[0])
    pick_rows(0)

    @pl.when(sp == 0)
    def _():
        for l in range(LAYERS):
            for q in range(2):
                ext[l, q, 0:HALO] = jnp.zeros((HALO, quarter), jnp.float32)

    ends = [has_up, has_down, swaps, follows(0), follows(1)]
    pl.semaphore_wait(barrier, 3 + sum(end.astype(jnp.int32) for end in ends))

    for half in range(gives(0)):
        vg_give(0, half).start()
    vg_own(0)
    loads[2].wait()
    x_peer(0).start()
    x_side().start()
    pick_rows(1)
    for half in range(gives(1)):
        vg_give(1, half).start()
    loads[3].wait()
    for l in range(LAYERS):
        pick_columns(l)
    for load in loads[4:]:
        load.wait()
    vg_side(0)
    for d in near:
        vg_line(0, d)
        if d == 1:
            x_peer(0).wait_recv()
            normalise_first(y)
            o_swapped(0)
            pl.when(last)(lambda: o_own_line(0, has_up, has_down))
            x_side().wait_recv()
            x_peer(1).start()
    pl.when(middle)(lambda: o_own_line(0, lower, upper))
    o_own_here(0)
    vg_line(0, levels - 1)
    x_peer(1).wait_recv()
    normalise_first(1 - y)
    vg_other(0)
    pl.when(middle)(lambda: o_own_line(0, upper, lower))
    glu(0)

    def o_near(l, *distances):
        for d in distances:
            o_line(l, d)

    pl.when(middle)(lambda: o_near(0, *near))
    vg_own(1)
    vg_side(1)
    o_swapped(1)
    pl.when(last)(lambda: o_own_line(1, has_up, has_down))
    conv(0, y)
    pl.when(last)(lambda: o_near(0, 1))
    take_glu(0)
    conv(0, 1 - y)
    o_across(0, step(0))
    pl.when(last)(lambda: o_near(0, *near[1:], levels - 1))
    activate(0, lambda: o_across(0, step(1)))
    project_first(step(0), 0)
    o_across(0, step(2))
    project_first(step(1), 1)
    pl.when(middle)(lambda: vg_line(1, 1))
    for i in range(2, levels):
        if i > 2:
            o_across(0, step(i))
        project_first(step(i), i)
    pl.when(last)(lambda: vg_line(1, 1))
    for i in range(0, levels, 2):
        landed(x1.at[0, 0, 0:2], x1sem.at[levels + i // 2])
        x1_diagonal(step(i + 1)).start()
        x1_side(step(i)).wait_recv()
        x1_peer(1, step(i), i).start()
        x1_side(step(i + 1)).wait_recv()
    for d in near[1:]:
        vg_line(1, d)
    normalise_next(y)
    pl.when(middle)(lambda: o_own_line(1, lower, upper))
    o_own_here(1)

    @pl.when(middle)
    def _():
        for d in near:
            o_line(1, d, lower, upper)

    for i in range(2):
        landed(x1.at[0, 0, 0:half_levels], x1sem.at[levels + half_levels + i])
    normalise_next(1 - y)
    vg_line(1, levels - 1)
    early = jnp.logical_and(last, core == 1)
    late = jnp.logical_and(last, core == 0)
    pl.when(early)(lambda: o_near(1, 2))
    vg_other(1)
    glu(1)

    @pl.when(middle)
    def _():
        for d in near:
            o_line(1, d, upper, lower)
        o_own_line(1, upper, lower)
        o_across(1, z)
        o_across_end(1)

    conv(1, y)
    pl.when(early)(lambda: o_near(1, *range(3, levels)))
    pl.when(late)(lambda: o_near(1, 2))
    take_glu(1)
    conv(1, 1 - y)
    pl.when(last)(lambda: o_across(1, z))
    pl.when(early)(lambda: o_near(1, 1))
    pl.when(late)(lambda: o_near(1, *range(3, levels)))
    at_end = last.astype(jnp.int32)

    def order(i):
        if i == 0:
            return step(0)
        return step(i + at_end if i < levels - 1 else levels - 1 - at_end * (levels - 2))

    pl.when(late)(lambda: o_across(1, order(1)))
    activate(1, lambda: None)
    squares = project_last(order(0))
    pl.when(late)(lambda: o_near(1, 1))

    @pl.when(core == 1)
    def _():
        for i in range(1, levels):
            o_across(1, order(i))

    for i in near[:-1]:
        pl.when(jnp.logical_and(middle, core == 0) if i == 1 else core == 0)(lambda: o_across(1, order(i)))
        squares = squares + project_last(order(i))
    pair = (order(levels - 2), order(levels - 1))
    squares = squares + project_pair(pair, y)

    @pl.when(core == 0)
    def _():
        for zz in pair:
            o_across(1, zz)

    squares = squares + project_pair(pair, 1 - y)
    st[...] = jnp.broadcast_to(squares, (rows, 128)).T[0:8]
    stat_copy().start()

    for zz in range(levels):
        @pl.when(z == zz)
        def _():
            for sem, count in ((upsem, zz + 1 if zz < levels - 1 else 0), (downsem, levels - zz if zz > 0 else 0)):
                count *= 3 * LAYERS
                extra = (zz == levels - 2) if sem is upsem else (zz == 1)
                if count:
                    landed(vg.at[0 : count + extra], sem)
    landed(vg.at[0 : 2 * n], coresem)
    count = LAYERS + LAYERS * levels + 2 + levels // 2 + levels // 4 + LAYERS // 2
    pl.when(middle)(lambda: landed(vg.at[0:count], sidesem))
    pl.when(last)(lambda: landed(vg.at[0 : count - 1], sidesem))
    pl.when(swaps)(lambda: landed(osw, swsem.at[0]))
    pl.when(follows(1))(lambda: landed(gl, hssem))
    pl.when(jnp.logical_not(follows(1)))(lambda: landed(gl.at[0], hssem))

    stat_copy().wait_recv()
    landed(x2r.at[0:half_levels], x2sem)
    both = st[...] + rst[...]
    total = jnp.concatenate([both] * (128 // 8), axis=0).T[:, 0:1]
    scale = lax.rsqrt(total / D + EPS)
    for i in range(half_levels):
        zz = tp * half_levels + i
        for part in range(2):
            for source, parity in ((x2, tp), (x2r, peer)):
                at = ((i * 2 + part) * 2 + parity) * width
                gain = fg_ref[0:1, pl.ds(pl.multiple_of(tp * cols + at, 128), width)]
                value = source[zz, part].astype(jnp.float32)
                out_ref[:, pl.ds(pl.multiple_of(at, 128), width)] = (value * scale * gain).astype(jnp.bfloat16)
    landed(vg.at[0 : 4 + levels // 2 + levels // 4 + LAYERS + levels // 4], xsem)
    stat_copy().wait_send()


def fused(n, stream, norm_gain, value_weight, gate_weight, conv_taps, ln_gain, ln_bias, out_weight, final_gain):
    rows, cols = stream.shape
    depth, ch = value_weight.shape[0] // LAYERS, value_weight.shape[1]
    width = out_weight.shape[1] // LAYERS
    levels = n // 4
    bf16, f32 = jnp.bfloat16, jnp.float32
    dma = pltpu.SemaphoreType.DMA
    arrays = (stream, norm_gain, value_weight, gate_weight, conv_taps.transpose(1, 0, 2),
              ln_gain, ln_bias, out_weight, final_gain.reshape(1, -1))
    return pl.pallas_call(
        functools.partial(fused_kernel, n),
        out_shape=pltpu.VMEM((rows, cols), bf16),
        in_specs=[pl.BlockSpec(memory_space=pl.ANY)] * 9,
        out_specs=pl.BlockSpec(memory_space=pltpu.VMEM),
        scratch_shapes=[pltpu.VMEM(array.shape, array.dtype) for array in arrays[1:]] + [
            dma((len(arrays) - 1,)),
            pltpu.VMEM((LAYERS * n, depth, ch), bf16),
            pltpu.VMEM((LAYERS, depth, ch), bf16),
            pltpu.VMEM((LAYERS, n, ch, width), bf16),
            pltpu.VMEM((LAYERS, ch, width), bf16),
            pltpu.VMEM((2, 2, rows, cols), bf16),
            pltpu.VMEM((2, 2, levels, 2, rows, width), bf16),
            pltpu.VMEM((levels, 2, rows, width), bf16),
            pltpu.VMEM((levels, 2, rows, width), bf16),
            pltpu.VMEM((2, rows, 2 * cols), bf16),
            pltpu.VMEM((LAYERS, 2, HALO, ch // 2), f32),
            pltpu.VMEM((LAYERS, rows, ch // 2), bf16),
            pltpu.VMEM((LAYERS, rows, ch // 2), bf16),
            pltpu.VMEM((LAYERS, 2, HALO + rows, ch // 2), f32),
            pltpu.VMEM((2, rows, ch // 2), f32),
            pltpu.VMEM((LAYERS, 2, rows, ch // 2), bf16),
            pltpu.VMEM((LAYERS, 2, rows, ch // 2), bf16),
            pltpu.VMEM((2, rows, ch), bf16),
            pltpu.VMEM((8, rows), f32),
            pltpu.VMEM((8, rows), f32),
            dma, dma, dma, dma, dma,
            dma((LAYERS + 1,)),
            dma((LAYERS, n // 2)),
            dma((LAYERS,)),
            dma((n // 2 + n,)),
            dma((levels + n // 2,)),
            dma((1 + LAYERS,)),
            dma((3,)),
            dma((levels + levels // 2 + 2,)),
            dma,
            dma((LAYERS,)),
            dma((LAYERS,)),
            dma,
            dma((LAYERS, 2)),
            dma((2,)),
        ],
        compiler_params=pltpu.CompilerParams(collective_id=0, has_side_effects=True),
    )(*arrays)


def solution(mesh):
    placed = (P("sp", "tp"), P(), P("sp", "tp"), P("sp", "tp"), P(), P(), P(), P("tp", "sp"), P())
    n, n_tp = mesh.shape["sp"], mesh.shape["tp"]

    def step(*args):
        stream, out_weight = args[0], args[7]
        fits = (n_tp == 2 and n % 8 == 0 and n > 8 and stream.shape[0] == 128 and out_weight.shape[1] == 128 * LAYERS
                and args[2].shape == (128 * LAYERS, 512))
        return fused(n, *args) if fits else local(*args)

    return jax.shard_map(step, mesh=mesh, in_specs=placed, out_specs=P("sp", "tp"), check_vma=False)
```
